32 devices in a mesh: grp: 2 (over y), sp: 4 (over z), tp: 4 (over x, core).
Axes of the slice: x: 2, y: 2, z: 4, core: 2. Of those that a mesh axis runs over, the one named last changes fastest.
Arguments:
- hidden_in: bfloat16 [5120, 4096], P(('grp', 'sp'), 'tp'), parts along dimension 0, may hold values from -64 to 64
- norm_gain: float32 [2, 4096], replicated, may hold values from 0.1 to 1.9
- w_pool_in: bfloat16 [2, 4096, 1024], P(None, 'sp', 'tp'), may hold values from -0.09375 to 0.09375
- w_pool_gate: bfloat16 [2, 4096, 1024], P(None, 'sp', 'tp'), may hold values from -0.09375 to 0.09375
- group_mix: bfloat16 [2, 16, 64, 64], replicated, may hold values from -0.75 to 0.75
- w_out: bfloat16 [2, 1024, 4096], P(None, 'sp', 'tp'), may hold values from -0.1875 to 0.1875
Outputs:
- hidden_out: bfloat16 [5120, 4096], P(('grp', 'sp'), 'tp'), parts along dimension 0
The draws below stay inside these ranges and needn't reach their ends.
There are 2 independent parts, one for each index of `grp`. The reference program is written for one: setup_inputs(seed, part) draws one part's arguments, and reference() takes and returns one part's arrays. A program takes and returns all parts, laid end to end along the dimension named above; an argument that names none is the same for every part. Nothing has to cross between parts.
All inputs are finite; a program needn't handle non-finite values.
Results may differ from the reference program's by a relative error of at most 0.012.
Values may be sent and summed in bfloat16 or wider, within the bound.
A program may use at most 64 MiB of HBM per device.

```python
import jax
import jax.numpy as jnp
from jax import lax

D = 4096
DP = 1024
GROUP = 64
GROUPS = 16
LAYERS = 2
TOKENS = 2560


def draw_hidden_in(key, part):
    base_key = jax.random.fold_in(key, 11)
    key_one, key_two = jax.random.split(base_key, 2)
    values = jax.random.normal(key_one, (TOKENS, D), jnp.float32)
    ramp = jnp.arange(D, dtype=jnp.float32) / D
    column_scale = jnp.exp(jnp.log(10.0) * (0.6 * ramp + 0.4 * jax.random.uniform(key_two, (D,), jnp.float32))) * 0.3162
    values = jnp.clip(values * column_scale[None, :], -60.0, 60.0)
    return values.astype(jnp.bfloat16)


def steps_of(key, extent, cuts, low, largest):
    loudness = 1.0
    for dim, parts in cuts:
        steps = jax.random.uniform(jax.random.fold_in(jax.random.fold_in(key, 6), dim), (parts,), jnp.float32, low / len(cuts), largest / len(cuts))
        loudness = loudness * jnp.repeat(jnp.exp(steps), extent[dim] // parts).reshape((-1,) + (1,) * (len(extent) - 1 - dim))
    return loudness


def scatter_about(rng, shape, scale, most, shards=(), kind=jnp.bfloat16):
    array = scale * jax.random.normal(rng, shape, jnp.float32)
    if shards:
        array = array * steps_of(rng, shape, shards, -0.22, 0.18)
    return jnp.clip(array, -most, most).astype(kind)


def setup_inputs(seed: int = 0, part: int = 0) -> dict:
    arg_keys = jax.random.split(jax.random.key(seed), 7)
    own_keys = jax.random.split(jax.random.fold_in(arg_keys[6], part), 7)
    hidden_in = draw_hidden_in(jax.random.fold_in(jax.random.fold_in(arg_keys[6], part), 71), part)
    norm_gain = jnp.clip(1.0 + 0.18 * jax.random.normal(arg_keys[1], (LAYERS, D), jnp.float32), 0.1, 1.9)
    w_pool_in = scatter_about(arg_keys[2], (LAYERS, D, DP), D ** -0.5, 0.09375, ((1, 4), (2, 4)))
    w_pool_gate = scatter_about(arg_keys[3], (LAYERS, D, DP), D ** -0.5, 0.09375, ((1, 4), (2, 4)))
    group_mix = scatter_about(arg_keys[4], (LAYERS, GROUPS, GROUP, GROUP), GROUP ** -0.5, 0.75)
    w_out = scatter_about(arg_keys[5], (LAYERS, DP, D), DP ** -0.5, 0.1875, ((1, 4), (2, 4)))
    return dict(hidden_in=hidden_in, norm_gain=norm_gain, w_pool_in=w_pool_in, w_pool_gate=w_pool_gate, group_mix=group_mix, w_out=w_out)


norm_eps = 1e-06

def reference(hidden_in, norm_gain, w_pool_in, w_pool_gate, group_mix, w_out):
    resid = hidden_in
    position = jnp.arange(TOKENS, dtype=jnp.int32)
    for layer in range(LAYERS):
        resid_f = resid.astype(jnp.float32)
        mean_sq = lax.optimization_barrier(jnp.mean(resid_f * resid_f, axis=1, keepdims=True))
        normed = (resid_f * lax.rsqrt(mean_sq + norm_eps) * norm_gain[layer]).astype(jnp.bfloat16)
        pool_in = jnp.dot(normed, w_pool_in[layer], preferred_element_type=jnp.float32).astype(jnp.bfloat16)
        gate = jnp.dot(normed, w_pool_gate[layer], preferred_element_type=jnp.float32).astype(jnp.bfloat16)
        grouped = pool_in.astype(jnp.float32).reshape(TOKENS, GROUPS, GROUP)
        running = jnp.concatenate([jnp.zeros((1, GROUPS, GROUP), jnp.float32), jnp.cumsum(grouped, axis=0)], axis=0)
        pieces = []
        for group_id in range(GROUPS):
            half = 2 ** (group_id % 4)
            lower = jnp.clip(position - half, 0, TOKENS).astype(jnp.int32)
            upper = jnp.clip(position + half, 0, TOKENS).astype(jnp.int32)
            window_sum = running[upper, group_id] - running[lower, group_id]
            counted = (upper - lower).astype(jnp.float32)[:, None]
            pieces.append(window_sum / counted - grouped[:, group_id])
        pooled = jnp.stack(pieces, axis=1).astype(jnp.bfloat16)
        mixed = jnp.einsum('tgc,gcd->tgd', pooled.astype(jnp.float32), group_mix[layer].astype(jnp.float32))
        mixed = mixed.reshape(TOKENS, DP)
        branch = (mixed * jax.nn.silu(gate.astype(jnp.float32))).astype(jnp.bfloat16)
        resid = (resid_f + jnp.dot(branch, w_out[layer], preferred_element_type=jnp.float32)).astype(jnp.bfloat16)
    return resid
```

```python
import functools

import jax
import jax.numpy as jnp
from jax import lax
from jax.experimental import pallas as pl
from jax.experimental.pallas import tpu as pltpu
from jax.sharding import PartitionSpec as P

GROUP = 64
HALO = 8
FULL = {(0, 0): ("inner",), (0, 1): ("inner",)}
NEAR = (0, 1, 3)
OUT_AFTER = 2
AHEAD = 2
MESH = pl.DeviceIdType.MESH

norm_eps = 1e-06


def guard(body, *conditions):
    traced = None
    for condition in conditions:
        if isinstance(condition, bool):
            if not condition:
                return
        else:
            traced = condition if traced is None else traced & condition
    if traced is None:
        body()
    else:
        pl.when(traced)(body)


def mixer(dims, h_in, gain, w_in, w_gate, mix, w_out, out, hg, hh, nb, nh, br, bh, wi, wg, wo, pad, acc_p, acc_g,
          gate_h, bd, local_sem, zr, zs, yr, ys, gr, gs, er, es, hs, tr, ts, pr, ps):
    sp_size, tp_size, layers, rows, cols, chans, chunks = dims
    step_rows = rows // chunks
    chips = tp_size // 2
    half = lax.axis_index("grp")
    row_rank = lax.axis_index("sp")
    rank = lax.axis_index("tp")
    chip, core = rank // 2, lax.rem(rank, 2)
    sibling = chip * 2 + 1 - core
    other = 1 - half
    total_rows = rows * sp_size
    last_row = sp_size - 1
    shards = ((w_in, wi), (w_gate, wg), (w_out, wo))
    up = jnp.minimum(row_rank + 1, last_row)
    down = jnp.maximum(row_rank - 1, 0)
    lower = row_rank < sp_size // 2
    at_end = (row_rank == 0) | (row_rank == last_row)
    host = True if sp_size == 4 else (row_rank == 1) | (row_rank == last_row - 1)
    inward = jnp.where(lower, up, down)
    outward = jnp.where(lower, down, up)

    def chip_rank(distance):
        return lax.rem(chip + distance, chips) * 2 + core

    def near(j):
        return j in NEAR

    def first(j):
        return pl.multiple_of(jnp.where(lower, chunks - 1 - j, j) * step_rows, step_rows)

    def span(j):
        return pl.ds(first(j), step_rows)

    own_w = {}
    for layer in range(layers):
        for t, (shard, whole) in enumerate(shards):
            depth = shard.shape[1]
            copy = pltpu.make_async_copy(
                shard.at[layer],
                whole.at[layer, pl.ds(pl.multiple_of(row_rank * depth, depth), depth)],
                local_sem.at[1 + layer * 3 + t],
            )
            copy.start()
            own_w[layer, t] = copy
    own_h = pltpu.make_async_copy(h_in, hg.at[0, rank], local_sem.at[0])
    own_h.start()

    barrier = pltpu.get_barrier_semaphore()
    peers = [
        {"sp": lax.rem(row_rank + 1, sp_size)},
        {"sp": lax.rem(row_rank + sp_size - 1, sp_size)},
        {"grp": other},
        {"tp": sibling},
    ] + [{"tp": chip_rank(d)} for d in range(1, chips)]
    for peer in peers:
        pl.semaphore_signal(barrier, inc=1, device_id=peer, device_id_type=MESH)
    pl.semaphore_wait(barrier, len(peers))

    streams = []
    for layer in range(layers):
        for t in range(3):
            streams.append((layer, t, "main"))
            streams.extend((layer, t, kind) for kind in FULL.get((layer, t), ()))

    def edge(q):
        return streams[q][0] == 0 and streams[q][1] < 2

    def member(kind, source):
        if kind == "inner":
            return (source > 0) & (source < last_row)
        if kind == "ends":
            return (source == 0) | (source == last_row)
        return True

    def swapped(layer, t, source):
        result = True
        for kind in FULL.get((layer, t), ()):
            absent = member(kind, source)
            absent = not absent if isinstance(absent, bool) else jnp.logical_not(absent)
            result = absent if result is True else result & absent
        return result

    def limits(q):
        return (1, last_row - 1) if edge(q) else (0, last_row)

    def piece_ref(layer, t, source, part):
        shard, whole = shards[t]
        depth = shard.shape[1]
        size = depth // 2
        start = pl.multiple_of(source * depth + part * size, size)
        return whole.at[layer, pl.ds(start, size)]

    def z_copy(q, source, to, send):
        layer, t, kind = streams[q]
        ref = piece_ref(layer, t, source, half if kind == "main" else other)
        return pltpu.make_async_remote_copy(
            ref, ref, zs.at[q, send], zr.at[q, source], device_id={"sp": to}, device_id_type=MESH
        )

    def y_copy(layer, t, source, part):
        ref = piece_ref(layer, t, source, part)
        return pltpu.make_async_remote_copy(
            ref, ref, ys.at[layer * 3 + t, source], yr.at[layer * 3 + t, source],
            device_id={"grp": other}, device_id_type=MESH,
        )

    def g_copy(kind, layer, j, source, to, send):
        ref = (hg, br)[kind].at[layer, source, span(j)]
        index = (kind * layers + layer) * chunks + j
        return pltpu.make_async_remote_copy(
            ref, ref, gs.at[index, send], gr.at[index, source], device_id={"tp": to}, device_id_type=MESH
        )

    def e_copy(j, source, to):
        return pltpu.make_async_remote_copy(
            hg.at[0, source, span(j)], hh.at[source, span(j)], es.at[j, source], er.at[j, source],
            device_id={"sp": to}, device_id_type=MESH,
        )

    def x_copy(j, source, to, send):
        ref = hh.at[source, span(j)]
        return pltpu.make_async_remote_copy(
            ref, ref, hs.at[j, send], er.at[j, source], device_id={"tp": to}, device_id_type=MESH
        )

    def t_copy(j, to):
        return pltpu.make_async_remote_copy(
            bh.at[span(j)], br.at[0, rank, span(j)], ts.at[j], tr.at[j], device_id={"sp": to}, device_id_type=MESH
        )

    def g_send(kind, layer, j):
        for d in range(1, chips):
            g_copy(kind, layer, j, rank, chip_rank(d), d).start()
        g_copy(kind, layer, j, rank, sibling, 0).start()

    def g_relay(kind, layer, j):
        for d in range(1, chips):
            source = chip_rank(d)
            g_copy(kind, layer, j, source, sibling, chips + d - 1).wait_recv()
            g_copy(kind, layer, j, source, sibling, chips + d - 1).start()

    def g_arrived(kind, layer, j):
        for d in range(chips):
            source = lax.rem(chip + d, chips) * 2 + 1 - core
            g_copy(kind, layer, j, source, sibling, 0).wait_recv()

    def g_sent(kind, layer, j):
        for d in range(1, chips):
            g_copy(kind, layer, j, rank, chip_rank(d), d).wait_send()
            g_copy(kind, layer, j, chip_rank(d), sibling, chips + d - 1).wait_send()
        g_copy(kind, layer, j, rank, sibling, 0).wait_send()

    def scaled(source, at, target, to, layer):
        squares = jnp.zeros((step_rows, 1), jnp.float32)
        for k in range(tp_size):
            block = source[k, at, :].astype(jnp.float32)
            squares = squares + jnp.sum(block * block, axis=1, keepdims=True)
        scaling = lax.rsqrt(squares / (cols * tp_size) + norm_eps)
        for k in range(tp_size):
            block = source[k, at, :].astype(jnp.float32)
            own_gain = gain[layer : layer + 1, k * cols : (k + 1) * cols]
            target[k, to, :] = (block * scaling * own_gain).astype(jnp.bfloat16)

    def normalize(layer, j):
        scaled(hg.at[layer], span(j), nb, span(j), layer)

    def project(acc, whole, layer):
        acc[...] = jnp.zeros_like(acc)

        @pl.loop(0, tp_size)
        def _(k):
            weight = whole[layer, pl.ds(pl.multiple_of(k * cols, cols), cols), :]
            acc[...] += jnp.dot(nb[k], weight, preferred_element_type=jnp.float32)

    def project_hosted(whole):
        total = jnp.zeros((step_rows, chans), jnp.float32)
        for k in range(tp_size):
            total = total + jnp.dot(nh[k], whole[0, k * cols : (k + 1) * cols, :], preferred_element_type=jnp.float32)
        return total.astype(jnp.bfloat16).astype(jnp.float32)

    own_shift = jnp.where(row_rank == 1, rows, 0)
    host_shift = jnp.where(row_rank == 1, 0, rows)
    groups = chans // GROUP

    def aligned(start):
        return pl.multiple_of(start, HALO)

    def halo_copy(layer, upward, shifted):
        if upward:
            source, target = rows + (own_shift if shifted else 0), 0
        else:
            source = HALO
            target = rows + HALO + (jnp.where(row_rank == 2, rows, 0) if shifted else 0)
        side = 0 if upward else 1
        return pltpu.make_async_remote_copy(
            pad.at[layer, pl.ds(aligned(source), HALO)], pad.at[layer, pl.ds(aligned(target), HALO)],
            ps.at[layer, side], pr.at[layer, side],
            device_id={"sp": up if upward else down}, device_id_type=MESH,
        )

    def halo_bounds(layer):
        return (1, last_row - 1) if layer == 0 else (0, last_row)

    def halo_send(layer):
        low, high = halo_bounds(layer)
        guard(lambda: halo_copy(layer, True, layer == 0).start(), row_rank < high)
        guard(lambda: halo_copy(layer, False, layer == 0).start(), row_rank > low)

    def halo_arrived(layer):
        low, high = halo_bounds(layer)
        guard(lambda: halo_copy(layer, True, False).wait_recv(), row_rank > low)
        guard(lambda: halo_copy(layer, False, False).wait_recv(), row_rank < high)

    def halo_sent(layer):
        low, high = halo_bounds(layer)
        guard(lambda: halo_copy(layer, True, False).wait_send(), row_rank < high)
        guard(lambda: halo_copy(layer, False, False).wait_send(), row_rank > low)

    def mix_matrix(layer):
        for g in range(groups):
            block = mix[layer, rank * groups + g].astype(jnp.float32)
            parts = [block if g == c else jnp.zeros((GROUP, GROUP), jnp.float32) for c in range(groups)]
            wide = parts[0] if groups == 1 else jnp.concatenate(parts, axis=1)
            bd[layer, g * GROUP : (g + 1) * GROUP, :] = wide.astype(jnp.bfloat16)

    def zero_pad(layer, start):
        pad[layer, start : start + HALO, :] = jnp.zeros((HALO, chans), jnp.float32)

    def gated(layer, j, shift, start, gate_ref):
        length = step_rows + 2 * HALO
        x = pad[layer, pl.ds(aligned(first(j) + shift), length), :]

        def ahead(v, n):
            return pltpu.roll(v, length - n, 0)

        sum1 = x + ahead(x, 1)
        sum2 = sum1 + ahead(sum1, 2)
        sum4 = sum2 + ahead(sum2, 4)
        sum8 = sum4 + ahead(sum4, 8)
        lane = lax.broadcasted_iota(jnp.int32, (step_rows, chans), 1)
        code = lax.rem(rank * groups + lane // GROUP, 4)
        position = start + first(j) + lax.broadcasted_iota(jnp.int32, (step_rows, chans), 0)
        running = jnp.where(
            code == 0, ahead(sum1, 7)[:step_rows],
            jnp.where(
                code == 1, ahead(sum2, 6)[:step_rows],
                jnp.where(code == 2, ahead(sum4, 4)[:step_rows], sum8[:step_rows]),
            ),
        )
        window = jnp.where(code == 0, 1, jnp.where(code == 1, 2, jnp.where(code == 2, 4, 8)))
        counted = (jnp.minimum(position + window, total_rows) - jnp.maximum(position - window, 0)).astype(jnp.float32)
        pooled = (running / counted - x[HALO : HALO + step_rows]).astype(jnp.bfloat16)
        mixed = jnp.dot(pooled, bd[layer], preferred_element_type=jnp.float32)
        gate = gate_ref[span(j), :].astype(jnp.bfloat16).astype(jnp.float32)
        return (mixed * (gate / (1.0 + jnp.exp(-gate)))).astype(jnp.bfloat16)

    def pool_chunk(layer, j):
        shift = own_shift if layer == 0 else 0
        br[layer, rank, span(j), :] = gated(layer, j, shift, row_rank * rows, acc_g)

    def pool_hosted(j):
        start = jnp.where(lower, row_rank - 1, row_rank + 1) * rows
        bh[span(j), :] = gated(0, j, host_shift, start, gate_h)
        t_copy(j, outward).start()

    def out_chunk(layer, j):
        total = hg[layer, rank, span(j), :].astype(jnp.float32)
        for k in range(tp_size):
            total = total + jnp.dot(
                br[layer, k, span(j), :], wo[layer, k * chans : (k + 1) * chans, :],
                preferred_element_type=jnp.float32,
            )
        if layer + 1 < layers:
            hg[layer + 1, rank, span(j), :] = total.astype(jnp.bfloat16)
        else:
            out[span(j), :] = total.astype(jnp.bfloat16)

    def y_wait(layer, t):
        for source in range(sp_size):
            guard(
                lambda source=source: y_copy(layer, t, source, other).wait_recv(),
                row_rank != source, swapped(layer, t, source),
            )

    def y_sent(layer, t):
        for source in range(sp_size):
            guard(
                lambda source=source: y_copy(layer, t, source, half).wait_send(),
                row_rank != source, swapped(layer, t, source),
            )

    def last_stream(layer, t):
        return max(q for q, stream in enumerate(streams) if stream[:2] == (layer, t))

    class Weights:
        def __init__(self, end):
            self.end = end
            self.loaded = set()
            self.owned = set()
            reach = range(1, sp_size) if end else range(1, last_row)
            order = [q for q in range(len(streams)) if not (end and edge(q))]
            if end:
                self.steps = [(q, 1) for q in order] + [(q, d) for q in order for d in reach if d > 1]
            else:
                self.steps = [(q, d) for q in order for d in reach]
            self.all = list(self.steps)

        def load(self, q):
            key = streams[q][:2]
            if key not in self.loaded:
                self.loaded.add(key)
                own_w[key].wait()

        def own(self, q, toward_end=False):
            kind = streams[q][2]
            low, high = limits(q)
            self.load(q)
            included = member(kind, row_rank)
            if self.end:
                guard(lambda: z_copy(q, row_rank, up, row_rank).start(), included, row_rank == 0)
                guard(lambda: z_copy(q, row_rank, down, sp_size).start(), included, row_rank == last_row)
                return
            if not toward_end and q in self.owned:
                return
            if not toward_end:
                self.owned.add(q)
            up_end, down_end = row_rank == last_row - 1, row_rank == 1
            if not toward_end:
                up_end, down_end = jnp.logical_not(up_end), jnp.logical_not(down_end)
            guard(lambda: z_copy(q, row_rank, up, row_rank).start(), included, row_rank + 1 <= high, up_end)
            guard(lambda: z_copy(q, row_rank, down, sp_size).start(), included, row_rank - 1 >= low, down_end)

        def step(self, q, distance):
            layer, t, kind = streams[q]
            bottom, top = limits(q)
            low, high = row_rank - distance, row_rank + distance

            def take(source, onward, to):
                copy = z_copy(q, source, to, source)
                copy.wait_recv()
                if not self.end:
                    guard(lambda: z_copy(q, source, to, source).start(), onward)
                if kind == "main":
                    guard(lambda: y_copy(layer, t, source, half).start(), swapped(layer, t, source))

            guard(lambda: take(low, row_rank + 1 <= top, up), low >= 0, member(kind, low))
            guard(lambda: take(high, row_rank - 1 >= bottom, down), high <= last_row, member(kind, high))

        def advance(self, count):
            while self.steps and len(self.all) - len(self.steps) < count:
                q, d = self.steps.pop(0)
                self.step(q, d)
                if not self.end and d == last_row - 1:
                    for later in range(q + 1, min(q + 1 + AHEAD, len(streams))):
                        self.own(later)

        def upto(self, layer, t, distance=None):
            q = last_stream(layer, t)
            reach = [d for p, d in self.all if p == q]
            self.advance(self.all.index((q, reach[-1] if distance is None else distance)) + 1)

        def arrived(self, layer, t):
            self.upto(layer, t)
            y_wait(layer, t)

        def finish(self):
            self.advance(len(self.all))
            for q, (layer, t, kind) in enumerate(streams):
                low, high = limits(q)
                if self.end:
                    included = member(kind, row_rank)
                    guard(lambda: z_copy(q, row_rank, up, row_rank).wait_send(), included, row_rank == 0)
                    guard(lambda: z_copy(q, row_rank, down, sp_size).wait_send(), included, row_rank == last_row)
                else:
                    for source in range(sp_size):
                        included = member(kind, source)
                        copy = z_copy(q, source, up, source)
                        guard(lambda: copy.wait_send(), included, source <= row_rank, row_rank + 1 <= high)
                        guard(lambda: copy.wait_send(), included, source > row_rank, row_rank - 1 >= low)
                    guard(
                        lambda: z_copy(q, row_rank, down, sp_size).wait_send(),
                        member(kind, row_rank), row_rank - 1 >= low,
                    )
                if kind == "main" and not (self.end and edge(q)):
                    y_sent(layer, t)

    def host_take(j):
        e_copy(j, rank, outward).wait_recv()
        if not near(j):
            for d in range(1, chips):
                x_copy(j, rank, chip_rank(d), d).start()
        x_copy(j, rank, sibling, chips).start()

    def host_relay(j):
        for d in range(1, chips):
            source = chip_rank(d)
            e_copy(j, source, outward).wait_recv()
            x_copy(j, source, sibling, chips + d).start()

    def host_arrived(j):
        for d in range(chips):
            source = lax.rem(chip + d, chips) * 2 + 1 - core
            e_copy(j, source, outward).wait_recv()

    def host_sent(j):
        if not near(j):
            for d in range(1, chips):
                x_copy(j, rank, chip_rank(d), d).wait_send()
        for d in range(chips):
            x_copy(j, chip_rank(d), sibling, chips + d).wait_send()
        t_copy(j, outward).wait_send()

    def host_project(j):
        scaled(hh, span(j), nh, pl.ds(0, step_rows), 0)
        pad[0, pl.ds(aligned(HALO + host_shift + first(j)), step_rows), :] = project_hosted(wi)
        gate_h[span(j), :] = project_hosted(wg)

    def own_project(weights, layer, shift):
        weights.arrived(layer, 0)
        project(acc_p, wi, layer)
        pad[layer, pl.ds(aligned(HALO + shift), rows), :] = acc_p[...].astype(jnp.bfloat16).astype(jnp.float32)
        halo_send(layer)

    def later_layers(weights, ready):
        for layer in range(1, layers):
            last = layer + 1 == layers
            for j in range(chunks):
                if layer == 1 and j < ready:
                    continue
                g_relay(0, layer, j)
                g_arrived(0, layer, j)
                normalize(layer, j)
            own_project(weights, layer, 0)
            weights.upto(layer, 1)
            weights.arrived(layer, 1)
            project(acc_g, wg, layer)
            weights.upto(layer, 2, 1)
            halo_arrived(layer)
            for j in range(chunks):
                pool_chunk(layer, j)
                g_send(1, layer, j)
            for j in range(chunks):
                g_relay(1, layer, j)
            weights.arrived(layer, 2)
            for j in range(chunks):
                g_arrived(1, layer, j)
                out_chunk(layer, j)
                if not last:
                    g_send(0, layer + 1, j)

    def all_sent(weights):
        weights.finish()
        for layer in range(1, layers):
            halo_sent(layer)
            for j in range(chunks):
                g_sent(0, layer, j)
                g_sent(1, layer, j)

    def end_program():
        weights = Weights(True)
        order = range(len(streams))
        for q in order:
            if edge(q):
                weights.own(q)
        own_h.wait()
        for j in range(chunks):
            if near(j):
                for d in range(1, chips):
                    g_copy(0, 0, j, rank, chip_rank(d), d).start()
        for j in range(chunks):
            e_copy(j, rank, inward).start()
            if near(j):
                for d in range(1, chips):
                    source = chip_rank(d)
                    g_copy(0, 0, j, source, sibling, 0).wait_recv()
                    e_copy(j, source, inward).start()
            if j == min(1, chunks - 1):
                for q in order:
                    if streams[q][:2] == (0, 2):
                        weights.own(q)
        for q in order:
            if not edge(q) and streams[q][:2] != (0, 2):
                weights.own(q)
        for layer in range(layers):
            mix_matrix(layer)
            if layer:
                guard(lambda: zero_pad(layer, 0), row_rank == 0)
                guard(lambda: zero_pad(layer, rows + HALO), row_rank == last_row)
        weights.advance(sum(1 for _, d in weights.all if d == 1))
        weights.arrived(0, 2)
        for j in range(chunks):
            t_copy(j, inward).wait_recv()
            g_send(1, 0, j)
            g_relay(1, 0, j)
            if j:
                g_relay(0, 1, j - 1)
            g_arrived(1, 0, j)
            out_chunk(0, j)
            g_send(0, 1, j)
            if j:
                g_arrived(0, 1, j - 1)
                normalize(1, j - 1)
        later_layers(weights, chunks - 1)
        all_sent(weights)
        for j in range(chunks):
            g_sent(1, 0, j)
            e_copy(j, rank, inward).wait_send()
            if near(j):
                for d in range(1, chips):
                    g_copy(0, 0, j, rank, chip_rank(d), d).wait_send()
                    e_copy(j, chip_rank(d), inward).wait_send()

    def mid_program():
        weights = Weights(False)
        own_h.wait()
        for q in range(1 + AHEAD):
            weights.own(q)
        for j in range(chunks):
            g_send(0, 0, j)
        for q in range(len(streams)):
            if not edge(q):
                weights.own(q, True)
        for layer in range(layers):
            mix_matrix(layer)
        guard(lambda: zero_pad(0, 0), row_rank == 1)
        guard(lambda: zero_pad(0, 2 * rows + HALO), row_rank == last_row - 1)
        entry = len([1 for q, _ in weights.all if edge(q)])
        for j in range(chunks):
            g_relay(0, 0, j)
            weights.advance(entry * (j + 1) // (chunks + 1))
            if j:
                g_arrived(0, 0, j - 1)
                normalize(0, j - 1)
        g_arrived(0, 0, chunks - 1)
        normalize(0, chunks - 1)
        guard(lambda: host_take(0), host)
        guard(lambda: host_relay(0), host)
        own_project(weights, 0, own_shift)
        weights.arrived(0, 1)
        project(acc_g, wg, 0)

        def own_pool():
            halo_arrived(0)
            for j in range(chunks):
                pool_chunk(0, j)
                g_send(1, 0, j)

        def own_out():
            for j in range(chunks):
                g_relay(1, 0, j)
            weights.arrived(0, 2)
            for j in range(chunks):
                g_arrived(1, 0, j)
                out_chunk(0, j)
                g_send(0, 1, j)

        tail = [q for q, d in weights.all if not edge(q)]
        for j in range(chunks):
            if j:
                guard(lambda: host_take(j), host)
                guard(lambda: host_relay(j), host)
            guard(lambda: host_arrived(j), host)
            guard(lambda: host_project(j), host)
            if j:
                guard(lambda: pool_hosted(j - 1), host)
            else:
                own_pool()
            if j == min(OUT_AFTER, chunks - 1):
                own_out()
            if j > OUT_AFTER:
                weights.upto(1, 0, 1 if j == OUT_AFTER + 1 else None)
        guard(lambda: pool_hosted(chunks - 1), host)
        later_layers(weights, 0)
        all_sent(weights)
        halo_sent(0)
        for j in range(chunks):
            g_sent(0, 0, j)
            g_sent(1, 0, j)
            guard(lambda: host_sent(j), host)

    pl.when(at_end)(end_program)
    pl.when(jnp.logical_not(at_end))(mid_program)


def solution(mesh):
    sp_size, tp_size = mesh.shape["sp"], mesh.shape["tp"]

    def local(hidden_in, norm_gain, w_pool_in, w_pool_gate, group_mix, w_out):
        rows, cols = hidden_in.shape
        layers, _, chans = w_pool_in.shape
        width, channels = cols * tp_size, chans * tp_size
        chunks = rows // 128 if tp_size <= 4 else 1
        streams = 3 * layers + sum(len(kinds) for kinds in FULL.values())
        dims = (sp_size, tp_size, layers, rows, cols, chans, chunks)
        bf16, f32 = jnp.bfloat16, jnp.float32
        dma = pltpu.SemaphoreType.DMA
        hbm, vmem = pl.BlockSpec(memory_space=pl.ANY), pl.BlockSpec(memory_space=pltpu.VMEM)
        return pl.pallas_call(
            functools.partial(mixer, dims),
            out_shape=jax.ShapeDtypeStruct((rows, cols), bf16),
            in_specs=[hbm, vmem, hbm, hbm, vmem, hbm],
            out_specs=vmem,
            scratch_shapes=[
                pltpu.VMEM((layers, tp_size, rows, cols), bf16),
                pltpu.VMEM((tp_size, rows, cols), bf16),
                pltpu.VMEM((tp_size, rows, cols), bf16),
                pltpu.VMEM((tp_size, rows // chunks, cols), bf16),
                pltpu.VMEM((layers, tp_size, rows, chans), bf16),
                pltpu.VMEM((rows, chans), bf16),
                pltpu.VMEM((layers, width, chans), bf16),
                pltpu.VMEM((layers, width, chans), bf16),
                pltpu.VMEM((layers, channels, cols), bf16),
                pltpu.VMEM((layers, 2 * rows + 2 * HALO, chans), f32),
                pltpu.VMEM((rows, chans), f32),
                pltpu.VMEM((rows, chans), f32),
                pltpu.VMEM((rows, chans), f32),
                pltpu.VMEM((layers, chans, chans), bf16),
                dma((1 + 3 * layers,)),
                dma((streams, sp_size)),
                dma((streams, sp_size + 1)),
                dma((3 * layers, sp_size)),
                dma((3 * layers, sp_size)),
                dma((2 * layers * chunks, tp_size)),
                dma((2 * layers * chunks, tp_size)),
                dma((chunks, tp_size)),
                dma((chunks, tp_size)),
                dma((chunks, tp_size)),
                dma((chunks,)),
                dma((chunks,)),
                dma((layers, 2)),
                dma((layers, 2)),
            ],
            compiler_params=pltpu.CompilerParams(
                collective_id=0, has_side_effects=True, vmem_limit_bytes=60 * 1024 * 1024
            ),
        )(hidden_in, norm_gain, w_pool_in, w_pool_gate, group_mix, w_out)

    in_specs = (
        P(("grp", "sp"), "tp"),
        P(),
        P(None, "sp", "tp"),
        P(None, "sp", "tp"),
        P(),
        P(None, "sp", "tp"),
    )
    out_specs = P(("grp", "sp"), "tp")
    return jax.shard_map(local, mesh=mesh, in_specs=in_specs, out_specs=out_specs, check_vma=False)
```

```python
import functools

import jax
import jax.numpy as jnp
from jax import lax
from jax.experimental import pallas as pl
from jax.experimental.pallas import tpu as pltpu
from jax.sharding import PartitionSpec as P

GROUP = 64
HALO = 8
FULL = {(0, 0): ("core",), (1, 0): ("near",), (1, 1): ("near",), (1, 2): ("near",)}
NEAR = (4,)
SEND = ('k', 'cs', 'k', 'k', 'k', 'ds', 'k', 'es', 'fs', 'ps', 'qs', 'rs')
EARLY = "cdef"
MID = ('ao', 'ai1', 'r', 'bo', 'bi1', 'xs', 'cs', 'r', 'n', 'ai', 'k', 'r', 'n', 'bi', 'co', 'r', 'n', 'k', 'xi', 'r', 'n', 'ci1', 'k', 'n', 'p', 'ds', 'g', 'ci', 'es', 'k', 'h', 'h', 'di1', 'o', 'h', 'do', 'h', 'fs', 'k', 'ei1', 'h', 'R', 'O', 'di', 'eo', 'fo', 'q', 'm', 'ei', 'fi1', 'q', 'm', 'fi', 'po', 'A', 'i', 'i', 'q', 'm', 'qo', 'i', 'E', 'e', 'e', 'e', 'q', 'm', 'i', 'e', 'b', 'b', 'b', 'ro', 'q', 'm', 'i', 'e', 'b', 'b', 'x', 'x', 'x', 'x', 'x', 'F', 'z', 'z', 'z', 'z', 'z')
END = ('ci1', 'di1', 'ei1', 'fi1', 'ci2', 'ci', 't', 't', 'Y', 'o', 'di2', 't', 'o', 't', 't', 'o', 'ei2', 'o', 'di', 'o', 'q', 'm', 'q', 'm', 'ei', 'q', 'm', 'A', 'i', 'i', 'i', 'fi2', 'q', 'm', 'i', 'E', 'e', 'e', 'b', 'e', 'b', 'fi', 'e', 'b', 'q', 'm', 'i', 'e', 'b', 'x', 'x', 'b', 'x', 'x', 'x', 'F', 'z', 'z', 'z', 'z', 'z')
MESH = pl.DeviceIdType.MESH

norm_eps = 1e-06


def guard(body, *conditions):
    traced = None
    for condition in conditions:
        if isinstance(condition, bool):
            if not condition:
                return
        else:
            traced = condition if traced is None else traced & condition
    if traced is None:
        body()
    else:
        pl.when(traced)(body)


def mixer(dims, h_in, gain, w_in, w_gate, mix, w_out, out, hg, hh, nb, nh, br, bh, wi, wg, wo, pad, acc_p, acc_g,
          gate_h, bd, local_sem, out_sem, zr, zs, yr, ys, gr, gs, er, es, hs, tr, ts, pr, ps):
    sp_size, tp_size, layers, rows, cols, chans, chunks = dims
    step_rows = rows // chunks
    chips = tp_size // 2
    half = lax.axis_index("grp")
    row_rank = lax.axis_index("sp")
    rank = lax.axis_index("tp")
    chip, core = rank // 2, lax.rem(rank, 2)
    sibling = chip * 2 + 1 - core
    other = 1 - half
    total_rows = rows * sp_size
    last_row = sp_size - 1
    shards = ((w_in, wi), (w_gate, wg), (w_out, wo))
    up = jnp.minimum(row_rank + 1, last_row)
    down = jnp.maximum(row_rank - 1, 0)
    lower = row_rank < sp_size // 2
    at_end = (row_rank == 0) | (row_rank == last_row)
    host = True if sp_size == 4 else (row_rank == 1) | (row_rank == last_row - 1)
    inward = jnp.where(lower, up, down)
    outward = jnp.where(lower, down, up)

    def chip_rank(distance):
        return lax.rem(chip + distance, chips) * 2 + core

    def near(j):
        return j in NEAR

    def first(j):
        return pl.multiple_of(jnp.where(lower, chunks - 1 - j, j) * step_rows, step_rows)

    def span(j):
        return pl.ds(first(j), step_rows)

    own_w = {}
    for layer in range(layers):
        for t, (shard, whole) in enumerate(shards):
            depth = shard.shape[1]
            copy = pltpu.make_async_copy(
                shard.at[layer],
                whole.at[layer, pl.ds(pl.multiple_of(row_rank * depth, depth), depth)],
                local_sem.at[1 + layer * 3 + t],
            )
            copy.start()
            own_w[layer, t] = copy
    own_h = pltpu.make_async_copy(h_in, hg.at[0, rank], local_sem.at[0])
    own_h.start()

    barrier = pltpu.get_barrier_semaphore()
    peers = [
        {"sp": lax.rem(row_rank + 1, sp_size)},
        {"sp": lax.rem(row_rank + sp_size - 1, sp_size)},
        {"grp": other},
        {"tp": sibling},
    ] + [{"tp": chip_rank(d)} for d in range(1, chips)]
    for peer in peers:
        pl.semaphore_signal(barrier, inc=1, device_id=peer, device_id_type=MESH)
    pl.semaphore_wait(barrier, len(peers))

    streams = [(layer, t, "main") for layer in range(layers) for t in range(3)]
    streams += [(layer, t, kind) for (layer, t), kinds in FULL.items() for kind in kinds]

    def edge(q):
        layer, t, kind = streams[q]
        return kind in ("core", "near") or (layer == 0 and t < 2)

    def member(kind, source):
        if kind in ("inner", "core"):
            return (source > 0) & (source < last_row)
        if kind == "near":
            return (source == 0) | (source == last_row)
        return True

    def swapped(layer, t, source, end):
        result = True
        for kind in FULL.get((layer, t), ()):
            if end and kind == "core":
                continue
            absent = member(kind, source)
            if kind == "near":
                absent = ((source == 0) & (row_rank == 1)) | ((source == last_row) & (row_rank == last_row - 1))
            absent = not absent if isinstance(absent, bool) else jnp.logical_not(absent)
            result = absent if result is True else result & absent
        return result

    def limits(q):
        return (1, last_row - 1) if edge(q) else (0, last_row)

    def piece_ref(layer, t, source, part):
        shard, whole = shards[t]
        depth = shard.shape[1]
        size = depth // 2
        start = pl.multiple_of(source * depth + part * size, size)
        return whole.at[layer, pl.ds(start, size)]

    def z_copy(q, source, to, send):
        layer, t, kind = streams[q]
        ref = piece_ref(layer, t, source, half if kind == "main" else other)
        return pltpu.make_async_remote_copy(
            ref, ref, zs.at[q, send], zr.at[q, source], device_id={"sp": to}, device_id_type=MESH
        )

    def y_copy(layer, t, source, part):
        ref = piece_ref(layer, t, source, part)
        return pltpu.make_async_remote_copy(
            ref, ref, ys.at[layer * 3 + t, source], yr.at[layer * 3 + t, source],
            device_id={"grp": other}, device_id_type=MESH,
        )

    def g_copy(kind, layer, j, source, to, send):
        ref = (hg, br)[kind].at[layer, source, span(j)]
        index = (kind * layers + layer) * chunks + j
        return pltpu.make_async_remote_copy(
            ref, ref, gs.at[kind * layers + layer, send], gr.at[index, source], device_id={"tp": to}, device_id_type=MESH
        )

    def e_copy(j, source, to):
        return pltpu.make_async_remote_copy(
            hg.at[0, source, span(j)], hh.at[source, span(j)], es.at[source], er.at[j, source],
            device_id={"sp": to}, device_id_type=MESH,
        )

    def x_copy(j, source, to, send):
        ref = hh.at[source, span(j)]
        return pltpu.make_async_remote_copy(
            ref, ref, hs.at[send], er.at[j, source], device_id={"tp": to}, device_id_type=MESH
        )

    def o_copy(j):
        return pltpu.make_async_copy(nb.at[0, span(j)], out.at[span(j)], out_sem.at[j])

    def t_copy(j, to):
        return pltpu.make_async_remote_copy(
            bh.at[span(j)], br.at[0, rank, span(j)], ts.at[0], tr.at[j], device_id={"sp": to}, device_id_type=MESH
        )

    def g_send(kind, layer, j):
        for d in range(1, chips):
            g_copy(kind, layer, j, rank, chip_rank(d), d).start()
        g_copy(kind, layer, j, rank, sibling, 0).start()

    def g_relay(kind, layer, j):
        for d in range(1, chips):
            source = chip_rank(d)
            g_copy(kind, layer, j, source, sibling, chips + d - 1).wait_recv()
            g_copy(kind, layer, j, source, sibling, chips + d - 1).start()

    def g_arrived(kind, layer, j):
        for d in range(chips):
            source = lax.rem(chip + d, chips) * 2 + 1 - core
            g_copy(kind, layer, j, source, sibling, 0).wait_recv()

    def flushed(ref, sem, count=chunks):
        if count:
            part = ref.at[pl.ds(0, count * step_rows)]
            pltpu.make_async_remote_copy(
                part, part, sem, gr.at[0, 0], device_id={"tp": sibling}, device_id_type=MESH
            ).wait_send()

    def g_sent(kind, layer):
        ref = (hg, br)[kind].at[layer, rank]
        for slot in range(2 * chips - 1):
            flushed(ref, gs.at[kind * layers + layer, slot])

    def scaled(source, at, target, to, layer):
        squares = jnp.zeros((step_rows, 1), jnp.float32)
        for k in range(tp_size):
            block = source[k, at, :].astype(jnp.float32)
            squares = squares + jnp.sum(block * block, axis=1, keepdims=True)
        scaling = lax.rsqrt(squares / (cols * tp_size) + norm_eps)
        for k in range(tp_size):
            block = source[k, at, :].astype(jnp.float32)
            own_gain = gain[layer : layer + 1, k * cols : (k + 1) * cols]
            target[k, to, :] = (block * scaling * own_gain).astype(jnp.bfloat16)

    def normalize(layer, j):
        scaled(hg.at[layer], span(j), nb, span(j), layer)

    def project(acc, whole, layer):
        acc[...] = jnp.zeros_like(acc)

        @pl.loop(0, tp_size)
        def _(k):
            weight = whole[layer, pl.ds(pl.multiple_of(k * cols, cols), cols), :]
            acc[...] += jnp.dot(nb[k], weight, preferred_element_type=jnp.float32)

    def project_hosted(whole):
        total = jnp.zeros((step_rows, chans), jnp.float32)
        for k in range(tp_size):
            total = total + jnp.dot(nh[k], whole[0, k * cols : (k + 1) * cols, :], preferred_element_type=jnp.float32)
        return total.astype(jnp.bfloat16).astype(jnp.float32)

    own_shift = jnp.where(row_rank == 1, rows, 0)
    host_shift = jnp.where(row_rank == 1, 0, rows)
    groups = chans // GROUP

    def aligned(start):
        return pl.multiple_of(start, HALO)

    def halo_copy(layer, upward, shifted):
        if upward:
            source, target = rows + (own_shift if shifted else 0), 0
        else:
            source = HALO
            target = rows + HALO + (jnp.where(row_rank == 2, rows, 0) if shifted else 0)
        side = 0 if upward else 1
        return pltpu.make_async_remote_copy(
            pad.at[layer, pl.ds(aligned(source), HALO)], pad.at[layer, pl.ds(aligned(target), HALO)],
            ps.at[layer, side], pr.at[layer, side],
            device_id={"sp": up if upward else down}, device_id_type=MESH,
        )

    def halo_bounds(layer):
        return (1, last_row - 1) if layer == 0 else (0, last_row)

    def halo_send(layer):
        low, high = halo_bounds(layer)
        guard(lambda: halo_copy(layer, True, layer == 0).start(), row_rank < high)
        guard(lambda: halo_copy(layer, False, layer == 0).start(), row_rank > low)

    def halo_side(layer, inner):
        low, high = halo_bounds(layer)
        rising = lower if inner else jnp.logical_not(lower)
        guard(lambda: halo_copy(layer, True, layer == 0).start(), rising, row_rank < high)
        guard(lambda: halo_copy(layer, False, layer == 0).start(), jnp.logical_not(rising), row_rank > low)

    def halo_arrived(layer):
        low, high = halo_bounds(layer)
        guard(lambda: halo_copy(layer, True, False).wait_recv(), row_rank > low)
        guard(lambda: halo_copy(layer, False, False).wait_recv(), row_rank < high)

    def halo_wait(layer, inner):
        rising = jnp.logical_not(lower) if inner else lower
        guard(lambda: halo_copy(layer, True, False).wait_recv(), rising, row_rank > 0)
        guard(lambda: halo_copy(layer, False, False).wait_recv(), jnp.logical_not(rising), row_rank < last_row)

    def halo_sent(layer):
        low, high = halo_bounds(layer)
        guard(lambda: halo_copy(layer, True, False).wait_send(), row_rank < high)
        guard(lambda: halo_copy(layer, False, False).wait_send(), row_rank > low)

    def mix_matrix(layer):
        for g in range(groups):
            block = mix[layer, rank * groups + g].astype(jnp.float32)
            parts = [block if g == c else jnp.zeros((GROUP, GROUP), jnp.float32) for c in range(groups)]
            wide = parts[0] if groups == 1 else jnp.concatenate(parts, axis=1)
            bd[layer, g * GROUP : (g + 1) * GROUP, :] = wide.astype(jnp.bfloat16)

    def zero_pad(layer, start):
        pad[layer, start : start + HALO, :] = jnp.zeros((HALO, chans), jnp.float32)

    def gated(layer, j, shift, start, gate_ref):
        length = step_rows + 2 * HALO
        x = pad[layer, pl.ds(aligned(first(j) + shift), length), :]

        def ahead(v, n):
            return pltpu.roll(v, length - n, 0)

        sum1 = x + ahead(x, 1)
        sum2 = sum1 + ahead(sum1, 2)
        sum4 = sum2 + ahead(sum2, 4)
        sum8 = sum4 + ahead(sum4, 8)
        lane = lax.broadcasted_iota(jnp.int32, (step_rows, chans), 1)
        code = lax.rem(rank * groups + lane // GROUP, 4)
        position = start + first(j) + lax.broadcasted_iota(jnp.int32, (step_rows, chans), 0)
        running = jnp.where(
            code == 0, ahead(sum1, 7)[:step_rows],
            jnp.where(
                code == 1, ahead(sum2, 6)[:step_rows],
                jnp.where(code == 2, ahead(sum4, 4)[:step_rows], sum8[:step_rows]),
            ),
        )
        window = jnp.where(code == 0, 1, jnp.where(code == 1, 2, jnp.where(code == 2, 4, 8)))
        counted = (jnp.minimum(position + window, total_rows) - jnp.maximum(position - window, 0)).astype(jnp.float32)
        pooled = (running / counted - x[HALO : HALO + step_rows]).astype(jnp.bfloat16)
        mixed = jnp.dot(pooled, bd[layer], preferred_element_type=jnp.float32)
        gate = gate_ref[span(j), :].astype(jnp.bfloat16).astype(jnp.float32)
        return (mixed * (gate / (1.0 + jnp.exp(-gate)))).astype(jnp.bfloat16)

    def pool_chunk(layer, j):
        shift = own_shift if layer == 0 else 0
        br[layer, rank, span(j), :] = gated(layer, j, shift, row_rank * rows, acc_g)

    def pool_hosted(j):
        start = jnp.where(lower, row_rank - 1, row_rank + 1) * rows
        bh[span(j), :] = gated(0, j, host_shift, start, gate_h)
        t_copy(j, outward).start()

    def out_chunk(layer, j):
        total = hg[layer, rank, span(j), :].astype(jnp.float32)
        for k in range(tp_size):
            total = total + jnp.dot(
                br[layer, k, span(j), :], wo[layer, k * chans : (k + 1) * chans, :],
                preferred_element_type=jnp.float32,
            )
        if layer + 1 < layers:
            hg[layer + 1, rank, span(j), :] = total.astype(jnp.bfloat16)
        else:
            nb[0, span(j), :] = total.astype(jnp.bfloat16)

    def y_wait(layer, t, end):
        for source in range(sp_size):
            guard(
                lambda source=source: y_copy(layer, t, source, other).wait_recv(),
                row_rank != source, swapped(layer, t, source, end),
            )

    def y_sent(layer, t, end):
        for source in range(sp_size):
            guard(
                lambda source=source: y_copy(layer, t, source, half).wait_send(),
                row_rank != source, swapped(layer, t, source, end),
            )

    names = {letter: (i // 3, i % 3, "main") for i, letter in enumerate("abcdef")}
    names.update(p=(1, 0, "near"), q=(1, 1, "near"), r=(1, 2, "near"), x=(0, 0, "core"), y=(0, 1, "core"), w=(0, 2, "inner"), v=(1, 0, "core"), u=(1, 1, "core"))

    class Weights:
        def __init__(self, end):
            self.end = end
            self.loaded = set()
            self.owned = set()
            self.done = set()

        def load(self, q):
            key = streams[q][:2]
            if key not in self.loaded:
                self.loaded.add(key)
                own_w[key].wait()

        def own(self, q, toward_end=False):
            kind = streams[q][2]
            low, high = limits(q)
            self.load(q)
            included = member(kind, row_rank)
            if not toward_end:
                if q in self.owned:
                    return
                self.owned.add(q)
            if self.end:
                guard(lambda: z_copy(q, row_rank, up, row_rank).start(), included, row_rank == 0)
                guard(lambda: z_copy(q, row_rank, down, sp_size).start(), included, row_rank == last_row)
                return
            up_end, down_end = row_rank == last_row - 1, row_rank == 1
            if not toward_end:
                up_end, down_end = jnp.logical_not(up_end), jnp.logical_not(down_end)
            guard(lambda: z_copy(q, row_rank, up, row_rank).start(), included, row_rank + 1 <= high, up_end)
            guard(lambda: z_copy(q, row_rank, down, sp_size).start(), included, row_rank - 1 >= low, down_end)

        def step(self, q, outer, distance):
            if (q, outer, distance) in self.done or (self.end and edge(q)):
                return
            self.done.add((q, outer, distance))
            layer, t, kind = streams[q]
            bottom, top = limits(q)
            below = lower if outer else jnp.logical_not(lower)
            source = jnp.where(below, row_rank - distance, row_rank + distance)
            onward = jnp.where(below, row_rank + 1 <= top, row_rank - 1 >= bottom)
            if kind == "near":
                if not outer or distance > 1:
                    return
                onward = False
            to = jnp.where(below, up, down)

            def take():
                z_copy(q, source, to, source).wait_recv()
                if not self.end:
                    guard(lambda: z_copy(q, source, to, source).start(), onward)
                if kind == "main":
                    guard(lambda: y_copy(layer, t, source, half).start(), swapped(layer, t, source, self.end))

            guard(take, source >= 0, source <= last_row, member(kind, source))

        def outer(self, q):
            if not self.end:
                for d in range(1, sp_size // 2):
                    self.step(q, True, d)

        def inner(self, q, reach=None):
            for d in range(1, (sp_size if self.end else sp_size - 1) if reach is None else reach + 1):
                self.step(q, False, d)

        def word(self, word):
            if names[word[0]] not in streams:
                return
            q = streams.index(names[word[0]])
            if word[1] == "s":
                self.own(q)
            elif word[1] == "o":
                self.outer(q)
            else:
                self.inner(q, int(word[2:]) if word[2:] else None)

        def settle(self, layer, t):
            for q, stream in enumerate(streams):
                if stream[:2] == (layer, t):
                    self.own(q)
                    self.outer(q)
                    self.inner(q)

        def arrived(self, layer, t):
            self.settle(layer, t)
            y_wait(layer, t, self.end)

        def finish(self):
            for q, (layer, t, kind) in enumerate(streams):
                low, high = limits(q)
                if self.end:
                    included = member(kind, row_rank)
                    guard(lambda: z_copy(q, row_rank, up, row_rank).wait_send(), included, row_rank == 0)
                    guard(lambda: z_copy(q, row_rank, down, sp_size).wait_send(), included, row_rank == last_row)
                elif kind != "near":
                    for source in range(sp_size):
                        included = member(kind, source)

                        def sent(source=source):
                            z_copy(q, source, up, source).wait_send()

                        guard(sent, included, source <= row_rank, row_rank + 1 <= high)
                        guard(sent, included, source > row_rank, row_rank - 1 >= low)
                    guard(
                        lambda: z_copy(q, row_rank, down, sp_size).wait_send(),
                        member(kind, row_rank), row_rank - 1 >= low,
                    )
                if kind == "main" and not (self.end and edge(q)):
                    y_sent(layer, t, self.end)

    def host_take(j):
        e_copy(j, rank, outward).wait_recv()
        if not near(j):
            for d in range(1, chips):
                x_copy(j, rank, chip_rank(d), d).start()
        x_copy(j, rank, sibling, chips).start()

    def host_relay(j):
        for d in range(1, chips):
            source = chip_rank(d)
            e_copy(j, source, outward).wait_recv()
            x_copy(j, source, sibling, chips + d).start()

    def host_arrived(j):
        for d in range(chips):
            source = lax.rem(chip + d, chips) * 2 + 1 - core
            e_copy(j, source, outward).wait_recv()

    few = sum(1 for j in range(chunks) if near(j))

    def host_sent():
        for d in range(1, chips):
            flushed(hh.at[rank], hs.at[d], chunks - few)
        for d in range(chips):
            flushed(hh.at[rank], hs.at[chips + d])
        flushed(bh, ts.at[0])

    def host_project(j):
        scaled(hh, span(j), nh, pl.ds(0, step_rows), 0)
        pad[0, pl.ds(aligned(HALO + host_shift + first(j)), step_rows), :] = project_hosted(wi)
        gate_h[span(j), :] = project_hosted(wg)

    def project_chunk(whole, layer, j):
        total = jnp.zeros((step_rows, chans), jnp.float32)
        for k in range(tp_size):
            weight = whole[layer, k * cols : (k + 1) * cols, :]
            total = total + jnp.dot(nb[k, span(j), :], weight, preferred_element_type=jnp.float32)
        return total

    def in_chunk(layer, j):
        rounded = project_chunk(wi, layer, j).astype(jnp.bfloat16).astype(jnp.float32)
        pad[layer, pl.ds(aligned(HALO + first(j)), step_rows), :] = rounded

    def gate_chunk(layer, j):
        acc_g[span(j), :] = project_chunk(wg, layer, j)

    def own_project(weights, layer, shift):
        weights.arrived(layer, 0)
        project(acc_p, wi, layer)
        pad[layer, pl.ds(aligned(HALO + shift), rows), :] = acc_p[...].astype(jnp.bfloat16).astype(jnp.float32)
        halo_send(layer)

    def emit_last(layer, j):
        g_arrived(1, layer, j)
        out_chunk(layer, j)
        if layer + 1 == layers:
            o_copy(j).start()
        else:
            g_send(0, layer + 1, j)

    def later_layers(weights):
        for layer in range(2, layers):
            weights.arrived(layer, 0)
            for j in range(chunks):
                g_relay(0, layer, j)
                g_arrived(0, layer, j)
                normalize(layer, j)
                in_chunk(layer, j)
            halo_side(layer, True)
            halo_side(layer, False)
            weights.arrived(layer, 1)
            halo_arrived(layer)
            for j in range(chunks):
                gate_chunk(layer, j)
                pool_chunk(layer, j)
                g_send(1, layer, j)
            for j in range(chunks):
                g_relay(1, layer, j)
            weights.arrived(layer, 2)
            for j in range(chunks):
                emit_last(layer, j)

    def second_layer(weights, end):
        def place(j):
            return j if end else chunks - 1 - j

        def ready(j):
            in_chunk(1, place(j))
            if place(j) == 0:
                halo_side(1, True)
            if place(j) == chunks - 1:
                halo_side(1, False)

        def branch(j):
            if place(j) == 0:
                halo_wait(1, True)
            if place(j) == chunks - 1 and not end:
                halo_wait(1, False)
            pool_chunk(1, place(j))
            g_send(1, 1, place(j))

        return {
            "q": lambda j: gather_next(place(j)), "m": lambda j: normalize_next(place(j)),
            "A": lambda j: weights.arrived(1, 0), "E": lambda j: weights.arrived(1, 1),
            "F": lambda j: weights.arrived(1, 2), "i": ready, "e": lambda j: gate_chunk(1, place(j)), "b": branch,
            "x": lambda j: g_relay(1, 1, place(j)), "z": lambda j: emit_last(1, place(j)),
        }

    def all_sent(weights):
        weights.finish()
        for layer in range(1, layers):
            halo_sent(layer)
            g_sent(0, layer)
            g_sent(1, layer)

    def run(script, weights, actions):
        counts = {}
        for word in script:
            if len(word) > 1:
                weights.word(word)
                continue
            j = counts.get(word, 0)
            counts[word] = j + 1
            if j < (1 if word in "pgoROYAEF" and word not in actions["many"] else chunks):
                actions[word](j)

    def gather_next(j):
        g_relay(0, 1, j)

    def normalize_next(j):
        g_arrived(0, 1, j)
        normalize(1, j)

    def end_program():
        weights = Weights(True)
        weights.own(0)
        weights.own(1)
        own_h.wait()
        for j in range(chunks):
            if near(j):
                for d in range(1, chips):
                    g_copy(0, 0, j, rank, chip_rank(d), d).start()

        def offer(j):
            e_copy(j, rank, inward).start()
            if near(j):
                for d in range(1, chips):
                    source = chip_rank(d)
                    g_copy(0, 0, j, source, sibling, 0).wait_recv()
                    e_copy(j, source, inward).start()

        run(SEND, weights, {"k": offer, "many": ""})
        for q in range(len(streams)):
            weights.own(q)
        for layer in range(layers):
            mix_matrix(layer)
            if layer:
                guard(lambda: zero_pad(layer, 0), row_rank == 0)
                guard(lambda: zero_pad(layer, rows + HALO), row_rank == last_row)

        def receive(j):
            t_copy(j, inward).wait_recv()
            g_send(1, 0, j)

        def emit(j):
            g_relay(1, 0, j)
            g_arrived(1, 0, j)
            out_chunk(0, j)
            g_send(0, 1, j)

        run(END, weights, {
            "t": receive, "o": emit, "Y": lambda j: weights.arrived(0, 2), "many": "o",
            **second_layer(weights, True),
        })
        later_layers(weights)
        all_sent(weights)
        g_sent(1, 0)
        flushed(hg.at[0, rank], es.at[rank])
        for d in range(1, chips):
            flushed(hg.at[0, rank], gs.at[0, d], few)
            flushed(hg.at[0, rank], es.at[chip_rank(d)], few)

    def mid_program():
        weights = Weights(False)
        weights.own(0)
        weights.own(1)
        own_h.wait()
        for j in range(chunks):
            g_send(0, 0, j)
        for letter in EARLY:
            weights.own(streams.index(names[letter]), True)
        for layer in range(layers):
            mix_matrix(layer)
        guard(lambda: zero_pad(0, 0), row_rank == 1)
        guard(lambda: zero_pad(0, 2 * rows + HALO), row_rank == last_row - 1)

        def normalize_own(j):
            g_arrived(0, 0, j)
            normalize(0, j)

        def gate(j):
            weights.arrived(0, 1)
            project(acc_g, wg, 0)

        def hosted(j):
            guard(lambda: host_relay(j), host)
            guard(lambda: host_arrived(j), host)
            guard(lambda: host_project(j), host)
            if j:
                guard(lambda: pool_hosted(j - 1), host)
            if j == chunks - 1:
                guard(lambda: pool_hosted(j), host)

        def own_pool(j):
            for i in reversed(range(chunks)):
                if i == 0:
                    halo_arrived(0)
                pool_chunk(0, i)
                g_send(1, 0, i)

        def relay_branch(j):
            for i in reversed(range(chunks)):
                g_relay(1, 0, i)

        def own_out(j):
            weights.arrived(0, 2)
            for i in reversed(range(chunks)):
                g_arrived(1, 0, i)
                out_chunk(0, i)
                g_send(0, 1, i)

        run(MID, weights, {
            "r": lambda j: g_relay(0, 0, j), "n": normalize_own, "k": lambda j: guard(lambda: host_take(j), host),
            "p": lambda j: own_project(weights, 0, own_shift), "g": gate, "h": hosted, "o": own_pool,
            "R": relay_branch, "O": own_out, "many": "", **second_layer(weights, False),
        })
        later_layers(weights)
        all_sent(weights)
        halo_sent(0)
        g_sent(0, 0)
        g_sent(1, 0)
        guard(host_sent, host)

    pl.when(at_end)(end_program)
    pl.when(jnp.logical_not(at_end))(mid_program)
    for j in range(chunks):
        o_copy(j).wait()


def solution(mesh):
    sp_size, tp_size = mesh.shape["sp"], mesh.shape["tp"]

    def local(hidden_in, norm_gain, w_pool_in, w_pool_gate, group_mix, w_out):
        rows, cols = hidden_in.shape
        layers, _, chans = w_pool_in.shape
        width, channels = cols * tp_size, chans * tp_size
        chunks = rows // 128 if tp_size <= 4 else 1
        streams = 3 * layers + sum(len(kinds) for kinds in FULL.values())
        dims = (sp_size, tp_size, layers, rows, cols, chans, chunks)
        bf16, f32 = jnp.bfloat16, jnp.float32
        dma = pltpu.SemaphoreType.DMA
        hbm, vmem = pl.BlockSpec(memory_space=pl.ANY), pl.BlockSpec(memory_space=pltpu.VMEM)
        return pl.pallas_call(
            functools.partial(mixer, dims),
            out_shape=jax.ShapeDtypeStruct((rows, cols), bf16),
            in_specs=[hbm, vmem, hbm, hbm, vmem, hbm],
            out_specs=hbm,
            scratch_shapes=[
                pltpu.VMEM((layers, tp_size, rows, cols), bf16),
                pltpu.VMEM((tp_size, rows, cols), bf16),
                pltpu.VMEM((tp_size, rows, cols), bf16),
                pltpu.VMEM((tp_size, rows // chunks, cols), bf16),
                pltpu.VMEM((layers, tp_size, rows, chans), bf16),
                pltpu.VMEM((rows, chans), bf16),
                pltpu.VMEM((layers, width, chans), bf16),
                pltpu.VMEM((layers, width, chans), bf16),
                pltpu.VMEM((layers, channels, cols), bf16),
                pltpu.VMEM((layers, 2 * rows + 2 * HALO, chans), f32),
                pltpu.VMEM((rows, chans), f32),
                pltpu.VMEM((rows, chans), f32),
                pltpu.VMEM((rows, chans), f32),
                pltpu.VMEM((layers, chans, chans), bf16),
                dma((1 + 3 * layers,)),
                dma((chunks,)),
                dma((streams, sp_size)),
                dma((streams, sp_size + 1)),
                dma((3 * layers, sp_size)),
                dma((3 * layers, sp_size)),
                dma((2 * layers * chunks, tp_size)),
                dma((2 * layers, tp_size)),
                dma((chunks, tp_size)),
                dma((tp_size,)),
                dma((tp_size,)),
                dma((chunks,)),
                dma((1,)),
                dma((layers, 2)),
                dma((layers, 2)),
            ],
            compiler_params=pltpu.CompilerParams(
                collective_id=0, has_side_effects=True, vmem_limit_bytes=60 * 1024 * 1024
            ),
        )(hidden_in, norm_gain, w_pool_in, w_pool_gate, group_mix, w_out)

    in_specs = (
        P(("grp", "sp"), "tp"),
        P(),
        P(None, "sp", "tp"),
        P(None, "sp", "tp"),
        P(),
        P(None, "sp", "tp"),
    )
    out_specs = P(("grp", "sp"), "tp")
    return jax.shard_map(local, mesh=mesh, in_specs=in_specs, out_specs=out_specs, check_vma=False)
```

```python
import functools

import jax
import jax.numpy as jnp
from jax import lax
from jax.experimental import pallas as pl
from jax.experimental.pallas import tpu as pltpu
from jax.sharding import PartitionSpec as P

GROUP = 64
HALO = 8
FULL = {(0, 0): ("core",), (1, 0): ("near",), (1, 1): ("near",), (1, 2): ("near",)}
NEAR = (4,)
SEND = ('k', 'cs', 'k', 'k', 'k', 'ds', 'k', 'es', 'fs', 'ps', 'qs', 'rs')
EARLY = "cdef"
MID = ('ao', 'ai1', 'r', 'bo', 'bi1', 'xs', 'cs', 'r', 'n', 'ai', 'k', 'r', 'n', 'bi', 'co', 'r', 'n', 'k', 'xi', 'r', 'n', 'ci1', 'k', 'n', 'p', 'ds', 'g', 'ci', 'es', 'k', 'h', 'h', 'di1', 'o', 'h', 'do', 'h', 'fs', 'ei1', 'R', 'O', 'k', 'h', 'di', 'eo', 'fo', 'q', 'm', 'ei', 'fi1', 'q', 'm', 'fi', 'po', 'A', 'i', 'i', 'q', 'm', 'qo', 'i', 'E', 'e', 'q', 'm', 'i', 'e', 'b', 'b', 'b', 'ro', 'q', 'm', 'i', 'e', 'b', 'b', 'x', 'x', 'x', 'x', 'F', 'z', 'z', 'x', 'z', 'z', 'z')
END = ('ci1', 'di1', 'ei1', 'fi1', 'ci2', 'ci', 't', 't', 'Y', 'o', 'di2', 't', 'o', 't', 't', 'o', 'ei2', 'o', 'di', 'o', 'q', 'm', 'q', 'm', 'ei', 'q', 'm', 'A', 'i', 'i', 'i', 'fi2', 'q', 'm', 'i', 'E', 'e', 'e', 'fi', 'b', 'b', 'b', 'q', 'm', 'i', 'e', 'b', 'b', 'x', 'x', 'x', 'x', 'F', 'z', 'z', 'x', 'z', 'z', 'z')
MESH = pl.DeviceIdType.MESH

norm_eps = 1e-06


def guard(body, *conditions):
    traced = None
    for condition in conditions:
        if isinstance(condition, bool):
            if not condition:
                return
        else:
            traced = condition if traced is None else traced & condition
    if traced is None:
        body()
    else:
        pl.when(traced)(body)


def mixer(dims, h_in, gain_in, w_in, w_gate, mix_in, w_out, out, gain, mix, hg, hh, nb, nh, br, bh, wi, wg, wo, pad, acc_p, acc_g,
          gate_h, bd, local_sem, out_sem, zr, zs, yr, ys, gr, gs, er, es, hs, tr, ts, pr, ps):
    sp_size, tp_size, layers, rows, cols, chans, chunks = dims
    step_rows = rows // chunks
    chips = tp_size // 2
    half = lax.axis_index("grp")
    row_rank = lax.axis_index("sp")
    rank = lax.axis_index("tp")
    chip, core = rank // 2, lax.rem(rank, 2)
    sibling = chip * 2 + 1 - core
    other = 1 - half
    total_rows = rows * sp_size
    last_row = sp_size - 1
    shards = ((w_in, wi), (w_gate, wg), (w_out, wo))
    up = jnp.minimum(row_rank + 1, last_row)
    down = jnp.maximum(row_rank - 1, 0)
    lower = row_rank < sp_size // 2
    at_end = (row_rank == 0) | (row_rank == last_row)
    host = True if sp_size == 4 else (row_rank == 1) | (row_rank == last_row - 1)
    inward = jnp.where(lower, up, down)
    outward = jnp.where(lower, down, up)

    def chip_rank(distance):
        return lax.rem(chip + distance, chips) * 2 + core

    def near(j):
        return j in NEAR

    def first(j):
        return pl.multiple_of(jnp.where(lower, chunks - 1 - j, j) * step_rows, step_rows)

    def span(j):
        return pl.ds(first(j), step_rows)

    own_w = {}
    for layer in range(layers):
        for t, (shard, whole) in enumerate(shards):
            depth = shard.shape[1]
            copy = pltpu.make_async_copy(
                shard.at[layer],
                whole.at[layer, pl.ds(pl.multiple_of(row_rank * depth, depth), depth)],
                local_sem.at[1 + layer * 3 + t],
            )
            copy.start()
            own_w[layer, t] = copy
    own_h = pltpu.make_async_copy(h_in, hg.at[0, rank], local_sem.at[0])
    own_h.start()

    own_gain = pltpu.make_async_copy(gain_in, gain, local_sem.at[1 + 3 * layers])
    own_mix = pltpu.make_async_copy(mix_in, mix, local_sem.at[2 + 3 * layers])
    own_gain.start()
    own_mix.start()

    barrier = pltpu.get_barrier_semaphore()
    peers = [
        {"sp": lax.rem(row_rank + 1, sp_size)},
        {"sp": lax.rem(row_rank + sp_size - 1, sp_size)},
        {"grp": other},
        {"tp": sibling},
    ] + [{"tp": chip_rank(d)} for d in range(1, chips)]
    for peer in peers:
        pl.semaphore_signal(barrier, inc=1, device_id=peer, device_id_type=MESH)
    pl.semaphore_wait(barrier, len(peers))

    streams = [(layer, t, "main") for layer in range(layers) for t in range(3)]
    streams += [(layer, t, kind) for (layer, t), kinds in FULL.items() for kind in kinds]

    def edge(q):
        layer, t, kind = streams[q]
        return kind in ("core", "near") or (layer == 0 and t < 2)

    def member(kind, source):
        if kind in ("inner", "core"):
            return (source > 0) & (source < last_row)
        if kind == "near":
            return (source == 0) | (source == last_row)
        return True

    def swapped(layer, t, source, end):
        result = True
        for kind in FULL.get((layer, t), ()):
            if end and kind == "core":
                continue
            absent = member(kind, source)
            if kind == "near":
                absent = ((source == 0) & (row_rank == 1)) | ((source == last_row) & (row_rank == last_row - 1))
            absent = not absent if isinstance(absent, bool) else jnp.logical_not(absent)
            result = absent if result is True else result & absent
        return result

    def limits(q):
        return (1, last_row - 1) if edge(q) else (0, last_row)

    def piece_ref(layer, t, source, part):
        shard, whole = shards[t]
        depth = shard.shape[1]
        size = depth // 2
        start = pl.multiple_of(source * depth + part * size, size)
        return whole.at[layer, pl.ds(start, size)]

    def z_copy(q, source, to, send):
        layer, t, kind = streams[q]
        ref = piece_ref(layer, t, source, half if kind == "main" else other)
        return pltpu.make_async_remote_copy(
            ref, ref, zs.at[q, send], zr.at[q, source], device_id={"sp": to}, device_id_type=MESH
        )

    def y_copy(layer, t, source, part):
        ref = piece_ref(layer, t, source, part)
        return pltpu.make_async_remote_copy(
            ref, ref, ys.at[layer * 3 + t, source], yr.at[layer * 3 + t, source],
            device_id={"grp": other}, device_id_type=MESH,
        )

    def g_copy(kind, layer, j, source, to, send):
        ref = (hg, br)[kind].at[layer, source, span(j)]
        index = (kind * layers + layer) * chunks + j
        return pltpu.make_async_remote_copy(
            ref, ref, gs.at[kind * layers + layer, send], gr.at[index, source], device_id={"tp": to}, device_id_type=MESH
        )

    def e_copy(j, source, to):
        return pltpu.make_async_remote_copy(
            hg.at[0, source, span(j)], hh.at[source, span(j)], es.at[source], er.at[j, source],
            device_id={"sp": to}, device_id_type=MESH,
        )

    def x_copy(j, source, to, send):
        ref = hh.at[source, span(j)]
        return pltpu.make_async_remote_copy(
            ref, ref, hs.at[send], er.at[j, source], device_id={"tp": to}, device_id_type=MESH
        )

    def o_copy(j):
        return pltpu.make_async_copy(nb.at[0, span(j)], out.at[span(j)], out_sem.at[j])

    def t_copy(j, to):
        return pltpu.make_async_remote_copy(
            bh.at[span(j)], br.at[0, rank, span(j)], ts.at[0], tr.at[j], device_id={"sp": to}, device_id_type=MESH
        )

    def g_send(kind, layer, j):
        for d in range(1, chips):
            g_copy(kind, layer, j, rank, chip_rank(d), d).start()
        g_copy(kind, layer, j, rank, sibling, 0).start()

    def g_relay(kind, layer, j):
        for d in range(1, chips):
            source = chip_rank(d)
            g_copy(kind, layer, j, source, sibling, chips + d - 1).wait_recv()
            g_copy(kind, layer, j, source, sibling, chips + d - 1).start()

    def g_arrived(kind, layer, j):
        for d in range(chips):
            source = lax.rem(chip + d, chips) * 2 + 1 - core
            g_copy(kind, layer, j, source, sibling, 0).wait_recv()

    def flushed(ref, sem, count=chunks):
        if count:
            part = ref.at[pl.ds(0, count * step_rows)]
            pltpu.make_async_remote_copy(
                part, part, sem, gr.at[0, 0], device_id={"tp": sibling}, device_id_type=MESH
            ).wait_send()

    def g_sent(kind, layer):
        ref = (hg, br)[kind].at[layer, rank]
        for slot in range(2 * chips - 1):
            flushed(ref, gs.at[kind * layers + layer, slot])

    def scaled(source, at, target, to, layer):
        squares = jnp.zeros((step_rows, 1), jnp.float32)
        for k in range(tp_size):
            block = source[k, at, :].astype(jnp.float32)
            squares = squares + jnp.sum(block * block, axis=1, keepdims=True)
        scaling = lax.rsqrt(squares / (cols * tp_size) + norm_eps)
        for k in range(tp_size):
            block = source[k, at, :].astype(jnp.float32)
            scale = gain[layer : layer + 1, k * cols : (k + 1) * cols]
            target[k, to, :] = (block * scaling * scale).astype(jnp.bfloat16)

    def normalize(layer, j):
        scaled(hg.at[layer], span(j), nb, span(j), layer)

    def project(acc, whole, layer):
        acc[...] = jnp.zeros_like(acc)

        @pl.loop(0, tp_size)
        def _(k):
            weight = whole[layer, pl.ds(pl.multiple_of(k * cols, cols), cols), :]
            acc[...] += jnp.dot(nb[k], weight, preferred_element_type=jnp.float32)

    def project_hosted(whole):
        total = jnp.zeros((step_rows, chans), jnp.float32)
        for k in range(tp_size):
            total = total + jnp.dot(nh[k], whole[0, k * cols : (k + 1) * cols, :], preferred_element_type=jnp.float32)
        return total.astype(jnp.bfloat16).astype(jnp.float32)

    own_shift = jnp.where(row_rank == 1, rows, 0)
    host_shift = jnp.where(row_rank == 1, 0, rows)
    groups = chans // GROUP

    def aligned(start):
        return pl.multiple_of(start, HALO)

    def halo_copy(layer, upward, shifted):
        if upward:
            source, target = rows + (own_shift if shifted else 0), 0
        else:
            source = HALO
            target = rows + HALO + (jnp.where(row_rank == 2, rows, 0) if shifted else 0)
        side = 0 if upward else 1
        return pltpu.make_async_remote_copy(
            pad.at[layer, pl.ds(aligned(source), HALO)], pad.at[layer, pl.ds(aligned(target), HALO)],
            ps.at[layer, side], pr.at[layer, side],
            device_id={"sp": up if upward else down}, device_id_type=MESH,
        )

    def halo_bounds(layer):
        return (1, last_row - 1) if layer == 0 else (0, last_row)

    def halo_send(layer):
        low, high = halo_bounds(layer)
        guard(lambda: halo_copy(layer, True, layer == 0).start(), row_rank < high)
        guard(lambda: halo_copy(layer, False, layer == 0).start(), row_rank > low)

    def halo_side(layer, inner):
        low, high = halo_bounds(layer)
        rising = lower if inner else jnp.logical_not(lower)
        guard(lambda: halo_copy(layer, True, layer == 0).start(), rising, row_rank < high)
        guard(lambda: halo_copy(layer, False, layer == 0).start(), jnp.logical_not(rising), row_rank > low)

    def halo_arrived(layer):
        low, high = halo_bounds(layer)
        guard(lambda: halo_copy(layer, True, False).wait_recv(), row_rank > low)
        guard(lambda: halo_copy(layer, False, False).wait_recv(), row_rank < high)

    def halo_wait(layer, inner):
        rising = jnp.logical_not(lower) if inner else lower
        guard(lambda: halo_copy(layer, True, False).wait_recv(), rising, row_rank > 0)
        guard(lambda: halo_copy(layer, False, False).wait_recv(), jnp.logical_not(rising), row_rank < last_row)

    def halo_sent(layer):
        low, high = halo_bounds(layer)
        guard(lambda: halo_copy(layer, True, False).wait_send(), row_rank < high)
        guard(lambda: halo_copy(layer, False, False).wait_send(), row_rank > low)

    def mix_matrix(layer):
        for g in range(groups):
            block = mix[layer, rank * groups + g].astype(jnp.float32)
            parts = [block if g == c else jnp.zeros((GROUP, GROUP), jnp.float32) for c in range(groups)]
            wide = parts[0] if groups == 1 else jnp.concatenate(parts, axis=1)
            bd[layer, g * GROUP : (g + 1) * GROUP, :] = wide.astype(jnp.bfloat16)

    def zero_pad(layer, start):
        pad[layer, start : start + HALO, :] = jnp.zeros((HALO, chans), jnp.float32)

    def gated(layer, j, shift, start, gate_ref):
        length = step_rows + 2 * HALO
        x = pad[layer, pl.ds(aligned(first(j) + shift), length), :]

        def ahead(v, n):
            return pltpu.roll(v, length - n, 0)

        sum1 = x + ahead(x, 1)
        sum2 = sum1 + ahead(sum1, 2)
        sum4 = sum2 + ahead(sum2, 4)
        sum8 = sum4 + ahead(sum4, 8)
        lane = lax.broadcasted_iota(jnp.int32, (step_rows, chans), 1)
        code = lax.rem(rank * groups + lane // GROUP, 4)
        position = start + first(j) + lax.broadcasted_iota(jnp.int32, (step_rows, chans), 0)
        running = jnp.where(
            code == 0, ahead(sum1, 7)[:step_rows],
            jnp.where(
                code == 1, ahead(sum2, 6)[:step_rows],
                jnp.where(code == 2, ahead(sum4, 4)[:step_rows], sum8[:step_rows]),
            ),
        )
        window = jnp.where(code == 0, 1, jnp.where(code == 1, 2, jnp.where(code == 2, 4, 8)))
        counted = (jnp.minimum(position + window, total_rows) - jnp.maximum(position - window, 0)).astype(jnp.float32)
        pooled = (running / counted - x[HALO : HALO + step_rows]).astype(jnp.bfloat16)
        mixed = jnp.dot(pooled, bd[layer], preferred_element_type=jnp.float32)
        gate = gate_ref[span(j), :].astype(jnp.bfloat16).astype(jnp.float32)
        return (mixed * (gate / (1.0 + jnp.exp(-gate)))).astype(jnp.bfloat16)

    def pool_chunk(layer, j):
        shift = own_shift if layer == 0 else 0
        br[layer, rank, span(j), :] = gated(layer, j, shift, row_rank * rows, acc_g)

    def pool_hosted(j):
        start = jnp.where(lower, row_rank - 1, row_rank + 1) * rows
        bh[span(j), :] = gated(0, j, host_shift, start, gate_h)
        t_copy(j, outward).start()

    def out_chunk(layer, j):
        total = hg[layer, rank, span(j), :].astype(jnp.float32)
        for k in range(tp_size):
            total = total + jnp.dot(
                br[layer, k, span(j), :], wo[layer, k * chans : (k + 1) * chans, :],
                preferred_element_type=jnp.float32,
            )
        if layer + 1 < layers:
            hg[layer + 1, rank, span(j), :] = total.astype(jnp.bfloat16)
        else:
            nb[0, span(j), :] = total.astype(jnp.bfloat16)

    def y_wait(layer, t, end):
        for source in range(sp_size):
            guard(
                lambda source=source: y_copy(layer, t, source, other).wait_recv(),
                row_rank != source, swapped(layer, t, source, end),
            )

    def y_sent(layer, t, end):
        for source in range(sp_size):
            guard(
                lambda source=source: y_copy(layer, t, source, half).wait_send(),
                row_rank != source, swapped(layer, t, source, end),
            )

    names = {letter: (i // 3, i % 3, "main") for i, letter in enumerate("abcdef")}
    names.update(p=(1, 0, "near"), q=(1, 1, "near"), r=(1, 2, "near"), x=(0, 0, "core"), y=(0, 1, "core"), w=(0, 2, "inner"), v=(1, 0, "core"), u=(1, 1, "core"))

    class Weights:
        def __init__(self, end):
            self.end = end
            self.loaded = set()
            self.owned = set()
            self.done = set()

        def load(self, q):
            key = streams[q][:2]
            if key not in self.loaded:
                self.loaded.add(key)
                own_w[key].wait()

        def own(self, q, toward_end=False):
            kind = streams[q][2]
            low, high = limits(q)
            self.load(q)
            included = member(kind, row_rank)
            if not toward_end:
                if q in self.owned:
                    return
                self.owned.add(q)
            if self.end:
                guard(lambda: z_copy(q, row_rank, up, row_rank).start(), included, row_rank == 0)
                guard(lambda: z_copy(q, row_rank, down, sp_size).start(), included, row_rank == last_row)
                return
            up_end, down_end = row_rank == last_row - 1, row_rank == 1
            if not toward_end:
                up_end, down_end = jnp.logical_not(up_end), jnp.logical_not(down_end)
            guard(lambda: z_copy(q, row_rank, up, row_rank).start(), included, row_rank + 1 <= high, up_end)
            guard(lambda: z_copy(q, row_rank, down, sp_size).start(), included, row_rank - 1 >= low, down_end)

        def step(self, q, outer, distance):
            if (q, outer, distance) in self.done or (self.end and edge(q)):
                return
            self.done.add((q, outer, distance))
            layer, t, kind = streams[q]
            bottom, top = limits(q)
            below = lower if outer else jnp.logical_not(lower)
            source = jnp.where(below, row_rank - distance, row_rank + distance)
            onward = jnp.where(below, row_rank + 1 <= top, row_rank - 1 >= bottom)
            if kind == "near":
                if not outer or distance > 1:
                    return
                onward = False
            to = jnp.where(below, up, down)

            def take():
                z_copy(q, source, to, source).wait_recv()
                if not self.end:
                    guard(lambda: z_copy(q, source, to, source).start(), onward)
                if kind == "main":
                    guard(lambda: y_copy(layer, t, source, half).start(), swapped(layer, t, source, self.end))

            guard(take, source >= 0, source <= last_row, member(kind, source))

        def outer(self, q):
            if not self.end:
                for d in range(1, sp_size // 2):
                    self.step(q, True, d)

        def inner(self, q, reach=None):
            for d in range(1, (sp_size if self.end else sp_size - 1) if reach is None else reach + 1):
                self.step(q, False, d)

        def word(self, word):
            if names[word[0]] not in streams:
                return
            q = streams.index(names[word[0]])
            if word[1] == "s":
                self.own(q)
            elif word[1] == "o":
                self.outer(q)
            else:
                self.inner(q, int(word[2:]) if word[2:] else None)

        def settle(self, layer, t):
            for q, stream in enumerate(streams):
                if stream[:2] == (layer, t):
                    self.own(q)
                    self.outer(q)
                    self.inner(q)

        def arrived(self, layer, t):
            self.settle(layer, t)
            y_wait(layer, t, self.end)

        def finish(self):
            for q, (layer, t, kind) in enumerate(streams):
                low, high = limits(q)
                if self.end:
                    included = member(kind, row_rank)
                    guard(lambda: z_copy(q, row_rank, up, row_rank).wait_send(), included, row_rank == 0)
                    guard(lambda: z_copy(q, row_rank, down, sp_size).wait_send(), included, row_rank == last_row)
                elif kind != "near":
                    for source in range(sp_size):
                        included = member(kind, source)

                        def sent(source=source):
                            z_copy(q, source, up, source).wait_send()

                        guard(sent, included, source <= row_rank, row_rank + 1 <= high)
                        guard(sent, included, source > row_rank, row_rank - 1 >= low)
                    guard(
                        lambda: z_copy(q, row_rank, down, sp_size).wait_send(),
                        member(kind, row_rank), row_rank - 1 >= low,
                    )
                if kind == "main" and not (self.end and edge(q)):
                    y_sent(layer, t, self.end)

    def host_take(j):
        e_copy(j, rank, outward).wait_recv()
        if not near(j):
            for d in range(1, chips):
                x_copy(j, rank, chip_rank(d), d).start()
        x_copy(j, rank, sibling, chips).start()

    def host_relay(j):
        for d in range(1, chips):
            source = chip_rank(d)
            e_copy(j, source, outward).wait_recv()
            x_copy(j, source, sibling, chips + d).start()

    def host_arrived(j):
        for d in range(chips):
            source = lax.rem(chip + d, chips) * 2 + 1 - core
            e_copy(j, source, outward).wait_recv()

    few = sum(1 for j in range(chunks) if near(j))

    def host_sent():
        for d in range(1, chips):
            flushed(hh.at[rank], hs.at[d], chunks - few)
        for d in range(chips):
            flushed(hh.at[rank], hs.at[chips + d])
        flushed(bh, ts.at[0])

    def host_project(j):
        scaled(hh, span(j), nh, pl.ds(0, step_rows), 0)
        pad[0, pl.ds(aligned(HALO + host_shift + first(j)), step_rows), :] = project_hosted(wi)
        gate_h[span(j), :] = project_hosted(wg)

    def project_chunk(whole, layer, j):
        total = jnp.zeros((step_rows, chans), jnp.float32)
        for k in range(tp_size):
            weight = whole[layer, k * cols : (k + 1) * cols, :]
            total = total + jnp.dot(nb[k, span(j), :], weight, preferred_element_type=jnp.float32)
        return total

    def in_chunk(layer, j):
        rounded = project_chunk(wi, layer, j).astype(jnp.bfloat16).astype(jnp.float32)
        pad[layer, pl.ds(aligned(HALO + first(j)), step_rows), :] = rounded

    def gate_rows(layer, at, count):
        total = jnp.zeros((count, chans), jnp.float32)
        for k in range(tp_size):
            weight = wg[layer, k * cols : (k + 1) * cols, :]
            total = total + jnp.dot(nb[k, at, :], weight, preferred_element_type=jnp.float32)
        acc_g[at, :] = total

    def own_project(weights, layer, shift):
        weights.arrived(layer, 0)
        project(acc_p, wi, layer)
        pad[layer, pl.ds(aligned(HALO + shift), rows), :] = acc_p[...].astype(jnp.bfloat16).astype(jnp.float32)
        halo_send(layer)

    def emit_last(layer, j):
        g_arrived(1, layer, j)
        out_chunk(layer, j)
        if layer + 1 == layers:
            o_copy(j).start()
        else:
            g_send(0, layer + 1, j)

    def later_layers(weights):
        for layer in range(2, layers):
            weights.arrived(layer, 0)
            for j in range(chunks):
                g_relay(0, layer, j)
                g_arrived(0, layer, j)
                normalize(layer, j)
                in_chunk(layer, j)
            halo_side(layer, True)
            halo_side(layer, False)
            weights.arrived(layer, 1)
            halo_arrived(layer)
            for j in range(chunks):
                gate_rows(layer, span(j), step_rows)
                pool_chunk(layer, j)
                g_send(1, layer, j)
            for j in range(chunks):
                g_relay(1, layer, j)
            weights.arrived(layer, 2)
            for j in range(chunks):
                emit_last(layer, j)

    def second_layer(weights, end):
        def place(j):
            return j if end else chunks - 1 - j

        def ready(j):
            in_chunk(1, place(j))
            if place(j) == 0:
                halo_side(1, True)
            if place(j) == chunks - 1:
                halo_side(1, False)

        def gate_pair(j):
            if 2 * j + 1 < chunks:
                begin = jnp.minimum(first(place(2 * j)), first(place(2 * j + 1)))
                gate_rows(1, pl.ds(pl.multiple_of(begin, step_rows), 2 * step_rows), 2 * step_rows)
            elif 2 * j < chunks:
                gate_rows(1, span(place(2 * j)), step_rows)

        def branch(j):
            if place(j) == 0:
                halo_wait(1, True)
            if place(j) == chunks - 1 and not end:
                halo_wait(1, False)
            pool_chunk(1, place(j))
            g_send(1, 1, place(j))

        return {
            "q": lambda j: gather_next(place(j)), "m": lambda j: normalize_next(place(j)),
            "A": lambda j: weights.arrived(1, 0), "E": lambda j: weights.arrived(1, 1),
            "F": lambda j: weights.arrived(1, 2), "i": ready, "e": gate_pair, "b": branch,
            "x": lambda j: g_relay(1, 1, place(j)), "z": lambda j: emit_last(1, place(j)),
        }

    def all_sent(weights):
        weights.finish()
        for layer in range(1, layers):
            halo_sent(layer)
            g_sent(0, layer)
            g_sent(1, layer)

    def run(script, weights, actions):
        counts = {}
        for word in script:
            if len(word) > 1:
                weights.word(word)
                continue
            j = counts.get(word, 0)
            counts[word] = j + 1
            if j < (1 if word in "pgoROYAEF" and word not in actions["many"] else chunks):
                actions[word](j)

    def gather_next(j):
        g_relay(0, 1, j)

    def normalize_next(j):
        g_arrived(0, 1, j)
        normalize(1, j)

    def end_program():
        weights = Weights(True)
        weights.own(0)
        weights.own(1)
        own_h.wait()
        for j in range(chunks):
            if near(j):
                for d in range(1, chips):
                    g_copy(0, 0, j, rank, chip_rank(d), d).start()

        def offer(j):
            e_copy(j, rank, inward).start()
            if near(j):
                for d in range(1, chips):
                    source = chip_rank(d)
                    g_copy(0, 0, j, source, sibling, 0).wait_recv()
                    e_copy(j, source, inward).start()

        run(SEND, weights, {"k": offer, "many": ""})
        for q in range(len(streams)):
            weights.own(q)
        own_gain.wait()
        own_mix.wait()
        for layer in range(layers):
            mix_matrix(layer)
            if layer:
                guard(lambda: zero_pad(layer, 0), row_rank == 0)
                guard(lambda: zero_pad(layer, rows + HALO), row_rank == last_row)

        def receive(j):
            t_copy(j, inward).wait_recv()
            g_send(1, 0, j)

        def emit(j):
            g_relay(1, 0, j)
            g_arrived(1, 0, j)
            out_chunk(0, j)
            g_send(0, 1, j)

        run(END, weights, {
            "t": receive, "o": emit, "Y": lambda j: weights.arrived(0, 2), "many": "o",
            **second_layer(weights, True),
        })
        later_layers(weights)
        all_sent(weights)
        g_sent(1, 0)
        flushed(hg.at[0, rank], es.at[rank])
        for d in range(1, chips):
            flushed(hg.at[0, rank], gs.at[0, d], few)
            flushed(hg.at[0, rank], es.at[chip_rank(d)], few)

    def mid_program():
        weights = Weights(False)
        weights.own(0)
        weights.own(1)
        own_h.wait()
        for j in range(chunks):
            g_send(0, 0, j)
        for letter in EARLY:
            weights.own(streams.index(names[letter]), True)
        own_gain.wait()
        own_mix.wait()
        for layer in range(layers):
            mix_matrix(layer)
        guard(lambda: zero_pad(0, 0), row_rank == 1)
        guard(lambda: zero_pad(0, 2 * rows + HALO), row_rank == last_row - 1)

        def normalize_own(j):
            g_arrived(0, 0, j)
            normalize(0, j)

        def gate(j):
            weights.arrived(0, 1)
            project(acc_g, wg, 0)

        def hosted(j):
            guard(lambda: host_relay(j), host)
            guard(lambda: host_arrived(j), host)
            guard(lambda: host_project(j), host)
            if j:
                guard(lambda: pool_hosted(j - 1), host)
            if j == chunks - 1:
                guard(lambda: pool_hosted(j), host)

        def own_pool(j):
            for i in reversed(range(chunks)):
                if i == 0:
                    halo_arrived(0)
                pool_chunk(0, i)
                g_send(1, 0, i)

        def relay_branch(j):
            for i in reversed(range(chunks)):
                g_relay(1, 0, i)

        def own_out(j):
            weights.arrived(0, 2)
            for i in reversed(range(chunks)):
                g_arrived(1, 0, i)
                out_chunk(0, i)
                g_send(0, 1, i)

        run(MID, weights, {
            "r": lambda j: g_relay(0, 0, j), "n": normalize_own, "k": lambda j: guard(lambda: host_take(j), host),
            "p": lambda j: own_project(weights, 0, own_shift), "g": gate, "h": hosted, "o": own_pool,
            "R": relay_branch, "O": own_out, "many": "", **second_layer(weights, False),
        })
        later_layers(weights)
        all_sent(weights)
        halo_sent(0)
        g_sent(0, 0)
        g_sent(1, 0)
        guard(host_sent, host)

    pl.when(at_end)(end_program)
    pl.when(jnp.logical_not(at_end))(mid_program)
    for j in range(chunks):
        o_copy(j).wait()


def solution(mesh):
    sp_size, tp_size = mesh.shape["sp"], mesh.shape["tp"]

    def local(hidden_in, norm_gain, w_pool_in, w_pool_gate, group_mix, w_out):
        rows, cols = hidden_in.shape
        layers, _, chans = w_pool_in.shape
        width, channels = cols * tp_size, chans * tp_size
        chunks = rows // 128 if tp_size <= 4 else 1
        streams = 3 * layers + sum(len(kinds) for kinds in FULL.values())
        dims = (sp_size, tp_size, layers, rows, cols, chans, chunks)
        bf16, f32 = jnp.bfloat16, jnp.float32
        dma = pltpu.SemaphoreType.DMA
        hbm = pl.BlockSpec(memory_space=pl.ANY)
        return pl.pallas_call(
            functools.partial(mixer, dims),
            out_shape=jax.ShapeDtypeStruct((rows, cols), bf16),
            in_specs=[hbm] * 6,
            out_specs=hbm,
            scratch_shapes=[
                pltpu.VMEM(norm_gain.shape, f32),
                pltpu.VMEM(group_mix.shape, bf16),
                pltpu.VMEM((layers, tp_size, rows, cols), bf16),
                pltpu.VMEM((tp_size, rows, cols), bf16),
                pltpu.VMEM((tp_size, rows, cols), bf16),
                pltpu.VMEM((tp_size, rows // chunks, cols), bf16),
                pltpu.VMEM((layers, tp_size, rows, chans), bf16),
                pltpu.VMEM((rows, chans), bf16),
                pltpu.VMEM((layers, width, chans), bf16),
                pltpu.VMEM((layers, width, chans), bf16),
                pltpu.VMEM((layers, channels, cols), bf16),
                pltpu.VMEM((layers, 2 * rows + 2 * HALO, chans), f32),
                pltpu.VMEM((rows, chans), f32),
                pltpu.VMEM((rows, chans), f32),
                pltpu.VMEM((rows, chans), f32),
                pltpu.VMEM((layers, chans, chans), bf16),
                dma((3 + 3 * layers,)),
                dma((chunks,)),
                dma((streams, sp_size)),
                dma((streams, sp_size + 1)),
                dma((3 * layers, sp_size)),
                dma((3 * layers, sp_size)),
                dma((2 * layers * chunks, tp_size)),
                dma((2 * layers, tp_size)),
                dma((chunks, tp_size)),
                dma((tp_size,)),
                dma((tp_size,)),
                dma((chunks,)),
                dma((1,)),
                dma((layers, 2)),
                dma((layers, 2)),
            ],
            compiler_params=pltpu.CompilerParams(
                collective_id=0, has_side_effects=True, vmem_limit_bytes=60 * 1024 * 1024
            ),
        )(hidden_in, norm_gain, w_pool_in, w_pool_gate, group_mix, w_out)

    in_specs = (
        P(("grp", "sp"), "tp"),
        P(),
        P(None, "sp", "tp"),
        P(None, "sp", "tp"),
        P(),
        P(None, "sp", "tp"),
    )
    out_specs = P(("grp", "sp"), "tp")
    return jax.shard_map(local, mesh=mesh, in_specs=in_specs, out_specs=out_specs, check_vma=False)
```

```python
import functools

import jax
import jax.numpy as jnp
from jax import lax
from jax.experimental import pallas as pl
from jax.experimental.pallas import tpu as pltpu
from jax.sharding import PartitionSpec as P

GROUP = 64
HALO = 8
FULL = {(0, 0): ("core",), (1, 0): ("near",), (1, 1): ("near",), (1, 2): ("near",)}
NEAR = (4,)
SEND = ('k', 'cs', 'k', 'k', 'k', 'ds', 'k', 'es', 'fs', 'ps', 'qs', 'rs')
EARLY = "cdef"
MID = ('ao', 'ai1', 'r', 'bo', 'bi1', 'xs', 'cs', 'r', 'n', 'ai', 'k', 'r', 'n', 'bi', 'co', 'r', 'n', 'k', 'xi', 'r', 'n', 'ci1', 'k', 'n', 'p', 'ds', 'g', 'ci', 'es', 'k', 'h', 'h', 'di1', 'o', 'h', 'do', 'h', 'fs', 'ei1', 'R', 'O', 'k', 'h', 'di', 'eo', 'fo', 'q', 'm', 'ei', 'fi1', 'q', 'm', 'fi', 'po', 'A', 'i', 'i', 'q', 'm', 'qo', 'i', 'E', 'e', 'q', 'm', 'i', 'e', 'b', 'b', 'b', 'ro', 'q', 'm', 'i', 'e', 'b', 'b', 'x', 'x', 'x', 'x', 'F', 'z', 'z', 'x', 'z', 'z', 'z')
END = ('ci1', 'di1', 'ei1', 'fi1', 'ci2', 'ci', 't', 't', 'Y', 'o', 'di2', 't', 'o', 't', 't', 'o', 'ei2', 'o', 'di', 'o', 'q', 'm', 'q', 'm', 'ei', 'q', 'm', 'A', 'i', 'i', 'i', 'fi2', 'q', 'm', 'i', 'E', 'e', 'e', 'fi', 'b', 'b', 'b', 'q', 'm', 'i', 'e', 'b', 'b', 'x', 'x', 'x', 'x', 'F', 'z', 'z', 'x', 'z', 'z', 'z')
MESH = pl.DeviceIdType.MESH

norm_eps = 1e-06


def guard(body, *conditions):
    traced = None
    for condition in conditions:
        if isinstance(condition, bool):
            if not condition:
                return
        else:
            traced = condition if traced is None else traced & condition
    if traced is None:
        body()
    else:
        pl.when(traced)(body)


def mixer(dims, h_in, gain_in, w_in, w_gate, mix_in, w_out, out, gain, mix, hg, hh, nb, nh, br, bh, wi, wg, wo, pad, acc_p, acc_g,
          gate_h, bd, local_sem, out_sem, zr, zs, yr, ys, gr, gs, er, es, hs, tr, ts, pr, ps):
    sp_size, tp_size, layers, rows, cols, chans, chunks = dims
    step_rows = rows // chunks
    chips = tp_size // 2
    half = lax.axis_index("grp")
    row_rank = lax.axis_index("sp")
    rank = lax.axis_index("tp")
    chip, core = rank // 2, lax.rem(rank, 2)
    sibling = chip * 2 + 1 - core
    other = 1 - half
    total_rows = rows * sp_size
    last_row = sp_size - 1
    shards = ((w_in, wi), (w_gate, wg), (w_out, wo))
    up = jnp.minimum(row_rank + 1, last_row)
    down = jnp.maximum(row_rank - 1, 0)
    lower = row_rank < sp_size // 2
    at_end = (row_rank == 0) | (row_rank == last_row)
    host = True if sp_size == 4 else (row_rank == 1) | (row_rank == last_row - 1)
    inward = jnp.where(lower, up, down)
    outward = jnp.where(lower, down, up)

    def chip_rank(distance):
        return lax.rem(chip + distance, chips) * 2 + core

    def near(j):
        return j in NEAR

    def first(j):
        return pl.multiple_of(jnp.where(lower, chunks - 1 - j, j) * step_rows, step_rows)

    def span(j):
        return pl.ds(first(j), step_rows)

    own_w = {}
    for layer in range(layers):
        for t, (shard, whole) in enumerate(shards):
            depth = shard.shape[1]
            copy = pltpu.make_async_copy(
                shard.at[layer],
                whole.at[layer, pl.ds(pl.multiple_of(row_rank * depth, depth), depth)],
                local_sem.at[1 + layer * 3 + t],
            )
            copy.start()
            own_w[layer, t] = copy
    own_h = pltpu.make_async_copy(h_in, hg.at[0, rank], local_sem.at[0])
    own_h.start()

    own_gain = pltpu.make_async_copy(gain_in, gain, local_sem.at[1 + 3 * layers])
    own_mix = pltpu.make_async_copy(mix_in, mix, local_sem.at[2 + 3 * layers])
    own_gain.start()
    own_mix.start()

    barrier = pltpu.get_barrier_semaphore()
    peers = [
        {"sp": lax.rem(row_rank + 1, sp_size)},
        {"sp": lax.rem(row_rank + sp_size - 1, sp_size)},
        {"grp": other},
        {"tp": sibling},
    ] + [{"tp": chip_rank(d)} for d in range(1, chips)]
    for peer in peers:
        pl.semaphore_signal(barrier, inc=1, device_id=peer, device_id_type=MESH)
    pl.semaphore_wait(barrier, len(peers))

    streams = [(layer, t, "main") for layer in range(layers) for t in range(3)]
    streams += [(layer, t, kind) for (layer, t), kinds in FULL.items() for kind in kinds]

    def edge(q):
        layer, t, kind = streams[q]
        return kind in ("core", "near") or (layer == 0 and t < 2)

    def member(kind, source):
        if kind in ("inner", "core"):
            return (source > 0) & (source < last_row)
        if kind == "near":
            return (source == 0) | (source == last_row)
        return True

    def swapped(layer, t, source, end):
        result = True
        for kind in FULL.get((layer, t), ()):
            if end and kind == "core":
                continue
            absent = member(kind, source)
            if kind == "near":
                absent = ((source == 0) & (row_rank == 1)) | ((source == last_row) & (row_rank == last_row - 1))
            absent = not absent if isinstance(absent, bool) else jnp.logical_not(absent)
            result = absent if result is True else result & absent
        return result

    def limits(q):
        return (1, last_row - 1) if edge(q) else (0, last_row)

    def piece_ref(layer, t, source, part):
        shard, whole = shards[t]
        depth = shard.shape[1]
        size = depth // 2
        start = pl.multiple_of(source * depth + part * size, size)
        return whole.at[layer, pl.ds(start, size)]

    def z_copy(q, source, to, send):
        layer, t, kind = streams[q]
        ref = piece_ref(layer, t, source, half if kind == "main" else other)
        return pltpu.make_async_remote_copy(
            ref, ref, zs.at[q], zr.at[q, source], device_id={"sp": to}, device_id_type=MESH
        )

    def y_copy(layer, t, source, part):
        ref = piece_ref(layer, t, source, part)
        return pltpu.make_async_remote_copy(
            ref, ref, ys.at[layer * 3 + t], yr.at[layer * 3 + t, source],
            device_id={"grp": other}, device_id_type=MESH,
        )

    def g_copy(kind, layer, j, source, to, send):
        ref = (hg, br)[kind].at[layer, source, span(j)]
        index = (kind * layers + layer) * chunks + j
        return pltpu.make_async_remote_copy(
            ref, ref, gs.at[kind * layers + layer, send], gr.at[index, source], device_id={"tp": to}, device_id_type=MESH
        )

    def e_copy(j, source, to):
        return pltpu.make_async_remote_copy(
            hg.at[0, source, span(j)], hh.at[source, span(j)], es.at[source], er.at[j, source],
            device_id={"sp": to}, device_id_type=MESH,
        )

    def x_copy(j, source, to, send):
        ref = hh.at[source, span(j)]
        return pltpu.make_async_remote_copy(
            ref, ref, hs.at[send], er.at[j, source], device_id={"tp": to}, device_id_type=MESH
        )

    def o_copy(j):
        return pltpu.make_async_copy(nb.at[0, span(j)], out.at[span(j)], out_sem.at[j])

    def t_copy(j, to):
        return pltpu.make_async_remote_copy(
            bh.at[span(j)], br.at[0, rank, span(j)], ts.at[0], tr.at[j], device_id={"sp": to}, device_id_type=MESH
        )

    def g_send(kind, layer, j):
        for d in range(1, chips):
            g_copy(kind, layer, j, rank, chip_rank(d), d).start()
        g_copy(kind, layer, j, rank, sibling, 0).start()

    def g_relay(kind, layer, j):
        for d in range(1, chips):
            source = chip_rank(d)
            g_copy(kind, layer, j, source, sibling, chips + d - 1).wait_recv()
            g_copy(kind, layer, j, source, sibling, chips + d - 1).start()

    def g_arrived(kind, layer, j):
        for d in range(chips):
            source = lax.rem(chip + d, chips) * 2 + 1 - core
            g_copy(kind, layer, j, source, sibling, 0).wait_recv()

    def flushed(ref, sem, count=chunks):
        if count:
            part = ref.at[pl.ds(0, count * step_rows)]
            pltpu.make_async_remote_copy(
                part, part, sem, gr.at[0, 0], device_id={"tp": sibling}, device_id_type=MESH
            ).wait_send()

    def g_sent(kind, layer):
        ref = (hg, br)[kind].at[layer, rank]
        for slot in range(2 * chips - 1):
            flushed(ref, gs.at[kind * layers + layer, slot])

    def scaled(source, at, target, to, layer):
        squares = jnp.zeros((step_rows, 1), jnp.float32)
        for k in range(tp_size):
            block = source[k, at, :].astype(jnp.float32)
            squares = squares + jnp.sum(block * block, axis=1, keepdims=True)
        scaling = lax.rsqrt(squares / (cols * tp_size) + norm_eps)
        for k in range(tp_size):
            block = source[k, at, :].astype(jnp.float32)
            scale = gain[layer : layer + 1, k * cols : (k + 1) * cols]
            target[k, to, :] = (block * scaling * scale).astype(jnp.bfloat16)

    def normalize(layer, j):
        scaled(hg.at[layer], span(j), nb, span(j), layer)

    def project(acc, whole, layer):
        acc[...] = jnp.zeros_like(acc)

        @pl.loop(0, tp_size)
        def _(k):
            weight = whole[layer, pl.ds(pl.multiple_of(k * cols, cols), cols), :]
            acc[...] += jnp.dot(nb[k], weight, preferred_element_type=jnp.float32)

    def project_hosted(whole):
        total = jnp.zeros((step_rows, chans), jnp.float32)
        for k in range(tp_size):
            total = total + jnp.dot(nh[k], whole[0, k * cols : (k + 1) * cols, :], preferred_element_type=jnp.float32)
        return total.astype(jnp.bfloat16).astype(jnp.float32)

    own_shift = jnp.where(row_rank == 1, rows, 0)
    host_shift = jnp.where(row_rank == 1, 0, rows)
    groups = chans // GROUP

    def aligned(start):
        return pl.multiple_of(start, HALO)

    def halo_copy(layer, upward, shifted):
        if upward:
            source, target = rows + (own_shift if shifted else 0), 0
        else:
            source = HALO
            target = rows + HALO + (jnp.where(row_rank == 2, rows, 0) if shifted else 0)
        side = 0 if upward else 1
        return pltpu.make_async_remote_copy(
            pad.at[layer, pl.ds(aligned(source), HALO)], pad.at[layer, pl.ds(aligned(target), HALO)],
            ps.at[layer, side], pr.at[layer, side],
            device_id={"sp": up if upward else down}, device_id_type=MESH,
        )

    def halo_bounds(layer):
        return (1, last_row - 1) if layer == 0 else (0, last_row)

    def halo_send(layer):
        low, high = halo_bounds(layer)
        guard(lambda: halo_copy(layer, True, layer == 0).start(), row_rank < high)
        guard(lambda: halo_copy(layer, False, layer == 0).start(), row_rank > low)

    def halo_side(layer, inner):
        low, high = halo_bounds(layer)
        rising = lower if inner else jnp.logical_not(lower)
        guard(lambda: halo_copy(layer, True, layer == 0).start(), rising, row_rank < high)
        guard(lambda: halo_copy(layer, False, layer == 0).start(), jnp.logical_not(rising), row_rank > low)

    def halo_arrived(layer):
        low, high = halo_bounds(layer)
        guard(lambda: halo_copy(layer, True, False).wait_recv(), row_rank > low)
        guard(lambda: halo_copy(layer, False, False).wait_recv(), row_rank < high)

    def halo_wait(layer, inner):
        rising = jnp.logical_not(lower) if inner else lower
        guard(lambda: halo_copy(layer, True, False).wait_recv(), rising, row_rank > 0)
        guard(lambda: halo_copy(layer, False, False).wait_recv(), jnp.logical_not(rising), row_rank < last_row)

    def halo_sent(layer):
        low, high = halo_bounds(layer)
        guard(lambda: halo_copy(layer, True, False).wait_send(), row_rank < high)
        guard(lambda: halo_copy(layer, False, False).wait_send(), row_rank > low)

    def mix_matrix(layer):
        for g in range(groups):
            block = mix[layer, rank * groups + g].astype(jnp.float32)
            parts = [block if g == c else jnp.zeros((GROUP, GROUP), jnp.float32) for c in range(groups)]
            wide = parts[0] if groups == 1 else jnp.concatenate(parts, axis=1)
            bd[layer, g * GROUP : (g + 1) * GROUP, :] = wide.astype(jnp.bfloat16)

    def zero_pad(layer, start):
        pad[layer, start : start + HALO, :] = jnp.zeros((HALO, chans), jnp.float32)

    def gated(layer, j, shift, start, gate_ref):
        length = step_rows + 2 * HALO
        x = pad[layer, pl.ds(aligned(first(j) + shift), length), :]

        def ahead(v, n):
            return pltpu.roll(v, length - n, 0)

        sum1 = x + ahead(x, 1)
        sum2 = sum1 + ahead(sum1, 2)
        sum4 = sum2 + ahead(sum2, 4)
        sum8 = sum4 + ahead(sum4, 8)
        lane = lax.broadcasted_iota(jnp.int32, (step_rows, chans), 1)
        code = lax.rem(rank * groups + lane // GROUP, 4)
        position = start + first(j) + lax.broadcasted_iota(jnp.int32, (step_rows, chans), 0)
        running = jnp.where(
            code == 0, ahead(sum1, 7)[:step_rows],
            jnp.where(
                code == 1, ahead(sum2, 6)[:step_rows],
                jnp.where(code == 2, ahead(sum4, 4)[:step_rows], sum8[:step_rows]),
            ),
        )
        window = jnp.where(code == 0, 1, jnp.where(code == 1, 2, jnp.where(code == 2, 4, 8)))
        counted = (jnp.minimum(position + window, total_rows) - jnp.maximum(position - window, 0)).astype(jnp.float32)
        pooled = (running / counted - x[HALO : HALO + step_rows]).astype(jnp.bfloat16)
        mixed = jnp.dot(pooled, bd[layer], preferred_element_type=jnp.float32)
        gate = gate_ref[span(j), :].astype(jnp.bfloat16).astype(jnp.float32)
        return (mixed * (gate / (1.0 + jnp.exp(-gate)))).astype(jnp.bfloat16)

    def pool_chunk(layer, j):
        shift = own_shift if layer == 0 else 0
        br[layer, rank, span(j), :] = gated(layer, j, shift, row_rank * rows, acc_g)

    def pool_hosted(j):
        start = jnp.where(lower, row_rank - 1, row_rank + 1) * rows
        bh[span(j), :] = gated(0, j, host_shift, start, gate_h)
        t_copy(j, outward).start()

    def out_chunk(layer, j):
        total = hg[layer, rank, span(j), :].astype(jnp.float32)
        for k in range(tp_size):
            total = total + jnp.dot(
                br[layer, k, span(j), :], wo[layer, k * chans : (k + 1) * chans, :],
                preferred_element_type=jnp.float32,
            )
        if layer + 1 < layers:
            hg[layer + 1, rank, span(j), :] = total.astype(jnp.bfloat16)
        else:
            nb[0, span(j), :] = total.astype(jnp.bfloat16)

    def y_wait(layer, t, end):
        for source in range(sp_size):
            guard(
                lambda source=source: y_copy(layer, t, source, other).wait_recv(),
                row_rank != source, swapped(layer, t, source, end),
            )

    names = {letter: (i // 3, i % 3, "main") for i, letter in enumerate("abcdef")}
    names.update(p=(1, 0, "near"), q=(1, 1, "near"), r=(1, 2, "near"), x=(0, 0, "core"), y=(0, 1, "core"), w=(0, 2, "inner"), v=(1, 0, "core"), u=(1, 1, "core"))

    class Weights:
        def __init__(self, end):
            self.end = end
            self.loaded = set()
            self.owned = set()
            self.done = set()

        def load(self, q):
            key = streams[q][:2]
            if key not in self.loaded:
                self.loaded.add(key)
                own_w[key].wait()

        def own(self, q, toward_end=False):
            kind = streams[q][2]
            low, high = limits(q)
            self.load(q)
            included = member(kind, row_rank)
            if not toward_end:
                if q in self.owned:
                    return
                self.owned.add(q)
            if self.end:
                guard(lambda: z_copy(q, row_rank, up, row_rank).start(), included, row_rank == 0)
                guard(lambda: z_copy(q, row_rank, down, sp_size).start(), included, row_rank == last_row)
                return
            up_end, down_end = row_rank == last_row - 1, row_rank == 1
            if not toward_end:
                up_end, down_end = jnp.logical_not(up_end), jnp.logical_not(down_end)
            guard(lambda: z_copy(q, row_rank, up, row_rank).start(), included, row_rank + 1 <= high, up_end)
            guard(lambda: z_copy(q, row_rank, down, sp_size).start(), included, row_rank - 1 >= low, down_end)

        def step(self, q, outer, distance):
            if (q, outer, distance) in self.done or (self.end and edge(q)):
                return
            self.done.add((q, outer, distance))
            layer, t, kind = streams[q]
            bottom, top = limits(q)
            below = lower if outer else jnp.logical_not(lower)
            source = jnp.where(below, row_rank - distance, row_rank + distance)
            onward = jnp.where(below, row_rank + 1 <= top, row_rank - 1 >= bottom)
            if kind == "near":
                if not outer or distance > 1:
                    return
                onward = False
            to = jnp.where(below, up, down)

            def take():
                z_copy(q, source, to, source).wait_recv()
                if not self.end:
                    guard(lambda: z_copy(q, source, to, source).start(), onward)
                if kind == "main":
                    guard(lambda: y_copy(layer, t, source, half).start(), swapped(layer, t, source, self.end))

            guard(take, source >= 0, source <= last_row, member(kind, source))

        def outer(self, q):
            if not self.end:
                for d in range(1, sp_size // 2):
                    self.step(q, True, d)

        def inner(self, q, reach=None):
            for d in range(1, (sp_size if self.end else sp_size - 1) if reach is None else reach + 1):
                self.step(q, False, d)

        def word(self, word):
            if names[word[0]] not in streams:
                return
            q = streams.index(names[word[0]])
            if word[1] == "s":
                self.own(q)
            elif word[1] == "o":
                self.outer(q)
            else:
                self.inner(q, int(word[2:]) if word[2:] else None)

        def settle(self, layer, t):
            for q, stream in enumerate(streams):
                if stream[:2] == (layer, t):
                    self.own(q)
                    self.outer(q)
                    self.inner(q)

        def arrived(self, layer, t):
            self.settle(layer, t)
            y_wait(layer, t, self.end)

        def finish(self):
            inside = False if host is True else jnp.logical_not(host)
            for q, (layer, t, kind) in enumerate(streams):
                shard, whole = shards[t]

                def flush(sem, count, *conditions, layer=layer, whole=whole, size=shard.shape[1] // 2):
                    part = whole.at[layer, pl.ds(0, count * size)]
                    guard(lambda: pltpu.make_async_remote_copy(
                        part, part, sem, zr.at[0, 0], device_id={"tp": sibling}, device_id_type=MESH
                    ).wait_send(), *conditions)

                swap = ys.at[layer * 3 + t]
                kinds = FULL.get((layer, t), ())
                if self.end:
                    if kind != "core":
                        flush(zs.at[q], 1)
                    if kind == "main" and not edge(q):
                        flush(swap, sp_size - 1)
                    continue
                if kind == "core":
                    flush(zs.at[q], 1, host)
                    flush(zs.at[q], sp_size - 1, inside)
                elif kind == "main":
                    flush(zs.at[q], 2 if edge(q) else sp_size + 1, host)
                    flush(zs.at[q], sp_size + 1, inside)
                    if "core" in kinds:
                        flush(swap, 2)
                    else:
                        flush(swap, sp_size - 2 if "near" in kinds else sp_size - 1, host)
                        flush(swap, sp_size - 1, inside)

    def host_take(j):
        e_copy(j, rank, outward).wait_recv()
        if not near(j):
            for d in range(1, chips):
                x_copy(j, rank, chip_rank(d), d).start()
        x_copy(j, rank, sibling, chips).start()

    def host_relay(j):
        for d in range(1, chips):
            source = chip_rank(d)
            e_copy(j, source, outward).wait_recv()
            x_copy(j, source, sibling, chips + d).start()

    def host_arrived(j):
        for d in range(chips):
            source = lax.rem(chip + d, chips) * 2 + 1 - core
            e_copy(j, source, outward).wait_recv()

    few = sum(1 for j in range(chunks) if near(j))

    def host_sent():
        for d in range(1, chips):
            flushed(hh.at[rank], hs.at[d], chunks - few)
        for d in range(chips):
            flushed(hh.at[rank], hs.at[chips + d])
        flushed(bh, ts.at[0])

    def host_project(j):
        scaled(hh, span(j), nh, pl.ds(0, step_rows), 0)
        pad[0, pl.ds(aligned(HALO + host_shift + first(j)), step_rows), :] = project_hosted(wi)
        gate_h[span(j), :] = project_hosted(wg)

    def project_chunk(whole, layer, j):
        total = jnp.zeros((step_rows, chans), jnp.float32)
        for k in range(tp_size):
            weight = whole[layer, k * cols : (k + 1) * cols, :]
            total = total + jnp.dot(nb[k, span(j), :], weight, preferred_element_type=jnp.float32)
        return total

    def in_chunk(layer, j):
        rounded = project_chunk(wi, layer, j).astype(jnp.bfloat16).astype(jnp.float32)
        pad[layer, pl.ds(aligned(HALO + first(j)), step_rows), :] = rounded

    def gate_rows(layer, at, count):
        total = jnp.zeros((count, chans), jnp.float32)
        for k in range(tp_size):
            weight = wg[layer, k * cols : (k + 1) * cols, :]
            total = total + jnp.dot(nb[k, at, :], weight, preferred_element_type=jnp.float32)
        acc_g[at, :] = total

    def own_project(weights, layer, shift):
        weights.arrived(layer, 0)
        project(acc_p, wi, layer)
        pad[layer, pl.ds(aligned(HALO + shift), rows), :] = acc_p[...].astype(jnp.bfloat16).astype(jnp.float32)
        halo_send(layer)

    def emit_last(layer, j):
        g_arrived(1, layer, j)
        out_chunk(layer, j)
        if layer + 1 == layers:
            o_copy(j).start()
        else:
            g_send(0, layer + 1, j)

    def later_layers(weights):
        for layer in range(2, layers):
            weights.arrived(layer, 0)
            for j in range(chunks):
                g_relay(0, layer, j)
                g_arrived(0, layer, j)
                normalize(layer, j)
                in_chunk(layer, j)
            halo_side(layer, True)
            halo_side(layer, False)
            weights.arrived(layer, 1)
            halo_arrived(layer)
            for j in range(chunks):
                gate_rows(layer, span(j), step_rows)
                pool_chunk(layer, j)
                g_send(1, layer, j)
            for j in range(chunks):
                g_relay(1, layer, j)
            weights.arrived(layer, 2)
            for j in range(chunks):
                emit_last(layer, j)

    def second_layer(weights, end):
        def place(j):
            return j if end else chunks - 1 - j

        def ready(j):
            in_chunk(1, place(j))
            if place(j) == 0:
                halo_side(1, True)
            if place(j) == chunks - 1:
                halo_side(1, False)

        def gate_pair(j):
            if 2 * j + 1 < chunks:
                begin = jnp.minimum(first(place(2 * j)), first(place(2 * j + 1)))
                gate_rows(1, pl.ds(pl.multiple_of(begin, step_rows), 2 * step_rows), 2 * step_rows)
            elif 2 * j < chunks:
                gate_rows(1, span(place(2 * j)), step_rows)

        def branch(j):
            if place(j) == 0:
                halo_wait(1, True)
            if place(j) == chunks - 1 and not end:
                halo_wait(1, False)
            pool_chunk(1, place(j))
            g_send(1, 1, place(j))

        return {
            "q": lambda j: gather_next(place(j)), "m": lambda j: normalize_next(place(j)),
            "A": lambda j: weights.arrived(1, 0), "E": lambda j: weights.arrived(1, 1),
            "F": lambda j: weights.arrived(1, 2), "i": ready, "e": gate_pair, "b": branch,
            "x": lambda j: g_relay(1, 1, place(j)), "z": lambda j: emit_last(1, place(j)),
        }

    def all_sent(weights):
        weights.finish()
        for layer in range(1, layers):
            halo_sent(layer)
            g_sent(0, layer)
            g_sent(1, layer)

    def run(script, weights, actions):
        counts = {}
        for word in script:
            if len(word) > 1:
                weights.word(word)
                continue
            j = counts.get(word, 0)
            counts[word] = j + 1
            if j < (1 if word in "pgoROYAEF" and word not in actions["many"] else chunks):
                actions[word](j)

    def gather_next(j):
        g_relay(0, 1, j)

    def normalize_next(j):
        g_arrived(0, 1, j)
        normalize(1, j)

    def end_program():
        weights = Weights(True)
        weights.own(0)
        weights.own(1)
        own_h.wait()
        for j in range(chunks):
            if near(j):
                for d in range(1, chips):
                    g_copy(0, 0, j, rank, chip_rank(d), d).start()

        def offer(j):
            e_copy(j, rank, inward).start()
            if near(j):
                for d in range(1, chips):
                    source = chip_rank(d)
                    g_copy(0, 0, j, source, sibling, 0).wait_recv()
                    e_copy(j, source, inward).start()

        run(SEND, weights, {"k": offer, "many": ""})
        for q in range(len(streams)):
            weights.own(q)
        own_gain.wait()
        own_mix.wait()
        for layer in range(layers):
            mix_matrix(layer)
            if layer:
                guard(lambda: zero_pad(layer, 0), row_rank == 0)
                guard(lambda: zero_pad(layer, rows + HALO), row_rank == last_row)

        def receive(j):
            t_copy(j, inward).wait_recv()
            g_send(1, 0, j)

        def emit(j):
            g_relay(1, 0, j)
            g_arrived(1, 0, j)
            out_chunk(0, j)
            g_send(0, 1, j)

        run(END, weights, {
            "t": receive, "o": emit, "Y": lambda j: weights.arrived(0, 2), "many": "o",
            **second_layer(weights, True),
        })
        later_layers(weights)
        all_sent(weights)
        g_sent(1, 0)
        flushed(hg.at[0, rank], es.at[rank])
        for d in range(1, chips):
            flushed(hg.at[0, rank], gs.at[0, d], few)
            flushed(hg.at[0, rank], es.at[chip_rank(d)], few)

    def mid_program():
        weights = Weights(False)
        weights.own(0)
        weights.own(1)
        own_h.wait()
        for j in range(chunks):
            g_send(0, 0, j)
        for letter in EARLY:
            weights.own(streams.index(names[letter]), True)
        own_gain.wait()
        own_mix.wait()
        for layer in range(layers):
            mix_matrix(layer)
        guard(lambda: zero_pad(0, 0), row_rank == 1)
        guard(lambda: zero_pad(0, 2 * rows + HALO), row_rank == last_row - 1)

        def normalize_own(j):
            g_arrived(0, 0, j)
            normalize(0, j)

        def gate(j):
            weights.arrived(0, 1)
            project(acc_g, wg, 0)

        def hosted(j):
            guard(lambda: host_relay(j), host)
            guard(lambda: host_arrived(j), host)
            guard(lambda: host_project(j), host)
            if j:
                guard(lambda: pool_hosted(j - 1), host)
            if j == chunks - 1:
                guard(lambda: pool_hosted(j), host)

        def own_pool(j):
            for i in reversed(range(chunks)):
                if i == 0:
                    halo_arrived(0)
                pool_chunk(0, i)
                g_send(1, 0, i)

        def relay_branch(j):
            for i in reversed(range(chunks)):
                g_relay(1, 0, i)

        def own_out(j):
            weights.arrived(0, 2)
            for i in reversed(range(chunks)):
                g_arrived(1, 0, i)
                out_chunk(0, i)
                g_send(0, 1, i)

        run(MID, weights, {
            "r": lambda j: g_relay(0, 0, j), "n": normalize_own, "k": lambda j: guard(lambda: host_take(j), host),
            "p": lambda j: own_project(weights, 0, own_shift), "g": gate, "h": hosted, "o": own_pool,
            "R": relay_branch, "O": own_out, "many": "", **second_layer(weights, False),
        })
        later_layers(weights)
        all_sent(weights)
        halo_sent(0)
        g_sent(0, 0)
        g_sent(1, 0)
        guard(host_sent, host)

    pl.when(at_end)(end_program)
    pl.when(jnp.logical_not(at_end))(mid_program)
    for j in range(chunks):
        o_copy(j).wait()


def solution(mesh):
    sp_size, tp_size = mesh.shape["sp"], mesh.shape["tp"]

    def local(hidden_in, norm_gain, w_pool_in, w_pool_gate, group_mix, w_out):
        rows, cols = hidden_in.shape
        layers, _, chans = w_pool_in.shape
        width, channels = cols * tp_size, chans * tp_size
        chunks = rows // 128 if tp_size <= 4 else 1
        streams = 3 * layers + sum(len(kinds) for kinds in FULL.values())
        dims = (sp_size, tp_size, layers, rows, cols, chans, chunks)
        bf16, f32 = jnp.bfloat16, jnp.float32
        dma = pltpu.SemaphoreType.DMA
        hbm = pl.BlockSpec(memory_space=pl.ANY)
        return pl.pallas_call(
            functools.partial(mixer, dims),
            out_shape=jax.ShapeDtypeStruct((rows, cols), bf16),
            in_specs=[hbm] * 6,
            out_specs=hbm,
            scratch_shapes=[
                pltpu.VMEM(norm_gain.shape, f32),
                pltpu.VMEM(group_mix.shape, bf16),
                pltpu.VMEM((layers, tp_size, rows, cols), bf16),
                pltpu.VMEM((tp_size, rows, cols), bf16),
                pltpu.VMEM((tp_size, rows, cols), bf16),
                pltpu.VMEM((tp_size, rows // chunks, cols), bf16),
                pltpu.VMEM((layers, tp_size, rows, chans), bf16),
                pltpu.VMEM((rows, chans), bf16),
                pltpu.VMEM((layers, width, chans), bf16),
                pltpu.VMEM((layers, width, chans), bf16),
                pltpu.VMEM((layers, channels, cols), bf16),
                pltpu.VMEM((layers, 2 * rows + 2 * HALO, chans), f32),
                pltpu.VMEM((rows, chans), f32),
                pltpu.VMEM((rows, chans), f32),
                pltpu.VMEM((rows, chans), f32),
                pltpu.VMEM((layers, chans, chans), bf16),
                dma((3 + 3 * layers,)),
                dma((chunks,)),
                dma((streams, sp_size)),
                dma((streams,)),
                dma((3 * layers, sp_size)),
                dma((3 * layers,)),
                dma((2 * layers * chunks, tp_size)),
                dma((2 * layers, tp_size)),
                dma((chunks, tp_size)),
                dma((tp_size,)),
                dma((tp_size,)),
                dma((chunks,)),
                dma((1,)),
                dma((layers, 2)),
                dma((layers, 2)),
            ],
            compiler_params=pltpu.CompilerParams(
                collective_id=0, has_side_effects=True, vmem_limit_bytes=60 * 1024 * 1024
            ),
        )(hidden_in, norm_gain, w_pool_in, w_pool_gate, group_mix, w_out)

    in_specs = (
        P(("grp", "sp"), "tp"),
        P(),
        P(None, "sp", "tp"),
        P(None, "sp", "tp"),
        P(),
        P(None, "sp", "tp"),
    )
    out_specs = P(("grp", "sp"), "tp")
    return jax.shard_map(local, mesh=mesh, in_specs=in_specs, out_specs=out_specs, check_vma=False)
```
